128 devices in a mesh: ep: 128 (over z, y, x, core).
Axes of the slice: x: 4, y: 4, z: 4, core: 2. Of those that a mesh axis runs over, the one named last changes fastest.
Arguments:
- tokens: bfloat16 [1536, 2048], P('ep'), may hold values from -6 to 6
- cache_latent: bfloat16 [1536, 1024, 512], P('ep'), may hold values from -180 to 180
- cache_rope: bfloat16 [1536, 1024, 64], P('ep'), may hold values from -6 to 6
- cache_lengths: int32 [1536], P('ep'), may hold values from 1 to 1024, as said below
- expert_ids: int32 [1536, 6], P('ep'), may hold values from 0 to 63, as said below
- route_weight: float32 [1536, 6], P('ep'), may hold values from 1 to 2
- attn_gain: float32 [2048], replicated, may hold values from 0.1 to 1.9
- q_gain: float32 [512], replicated, may hold values from 0.1 to 1.9
- kv_gain: float32 [512], replicated, may hold values from 0.1 to 1.9
- moe_gain: float32 [2048], replicated, may hold values from 0.1 to 1.9
- w_qdown: bfloat16 [2048, 512], replicated, may hold values from -0.125 to 0.125
- w_kvdown: bfloat16 [2048, 512], replicated, may hold values from -0.125 to 0.125
- w_krope: bfloat16 [2048, 64], replicated, may hold values from -0.125 to 0.125
- w_qup: bfloat16 [512, 1536], replicated, may hold values from -0.25 to 0.25
- w_kup: bfloat16 [512, 1024], replicated, may hold values from -0.5 to 0.5
- w_vup: bfloat16 [512, 1024], replicated, may hold values from -0.25 to 0.25
- w_out: bfloat16 [1024, 2048], replicated, may hold values from -0.1875 to 0.1875
- expert_gate: bfloat16 [128, 2048, 256], P('ep'), may hold values from -0.125 to 0.125
- expert_up: bfloat16 [128, 2048, 256], P('ep'), may hold values from -0.125 to 0.125
- expert_down: bfloat16 [128, 256, 2048], P('ep'), may hold values from -0.25 to 0.25
Outputs:
- mixed: float32 [1536, 2048], P('ep')
- new_latent: bfloat16 [1536, 512], P('ep')
- new_rope_key: bfloat16 [1536, 64], P('ep')
The draws below stay inside these ranges and needn't reach their ends.
Inputs may be any that keep to these rules, and one draw needn't show every extreme that they name: `cache_lengths`: some sequence holds 1024 positions. `expert_ids`: each row names 6 different experts of one group g, numbered g * 16 to g * 16 + 15; among the rows of one device no expert is named more than 3 times, and some expert exactly 3 times.
All inputs are finite; a program needn't handle non-finite values.
Results may differ from the reference program's by a relative error of at most 0.03.
Values may be sent and summed in bfloat16 or wider, within the bound.
A program may use at most 128 MiB of HBM per device.

```python
import jax
import jax.numpy as jnp
from jax import lax

D = 2048
HEADS = 8
Q_RANK = 512
KV_RANK = 512
NOPE_DIM = 128
ROPE_DIM = 64
VALUE_DIM = 128
FF = 512
GROUP_SIZE = 16
TOP_K = 6
SEQ_DEV = 12
CACHE = 1024
TOKENS = 1536
EXPERTS = 64
GROUPS = 4
GROUP_MOST = 6
CAPACITY = 3
N_EP = 128


def draw_cache_lengths(key, part):
    block_count = TOKENS // SEQ_DEV
    key_list = jax.random.split(jax.random.fold_in(key, 7), 2)
    factor = jax.random.randint(key_list[0], (block_count, 1), 1, 5)
    upper_bound = CACHE * factor // 4
    raw_bits = jax.random.randint(key_list[1], (block_count, SEQ_DEV), 0, 1 << 30)
    lengths = (1 + raw_bits % upper_bound).reshape(TOKENS)
    lengths = lengths.at[0].set(CACHE)
    return lengths.astype(jnp.int32)


def draw_expert_ids(key, part):
    block_count = TOKENS // SEQ_DEV
    base_key = jax.random.fold_in(key, 13)
    seq_order = jax.vmap(lambda sub_key: jax.random.permutation(sub_key, SEQ_DEV))(jax.random.split(jax.random.fold_in(base_key, 1), block_count))
    group_order = jax.vmap(lambda sub_key: jax.random.permutation(sub_key, GROUPS))(jax.random.split(jax.random.fold_in(base_key, 2), block_count))
    local_table = jax.vmap(lambda sub_key: jax.random.permutation(sub_key, GROUP_SIZE))(jax.random.split(jax.random.fold_in(base_key, 3), block_count * GROUPS)).reshape(block_count, GROUPS, GROUP_SIZE)
    others = max(GROUPS - 1, 1)
    first_run = seq_order < GROUP_MOST
    rest_rank = jnp.maximum(seq_order - GROUP_MOST, 0)
    slot_index = jnp.where(first_run, 0, 1 + rest_rank % others)
    group_rank = jnp.where(first_run, seq_order, rest_rank // others)
    group_ids = jnp.take_along_axis(group_order, slot_index, axis=1)
    spot_index = (group_rank[:, :, None] * TOP_K + jnp.arange(TOP_K, dtype=jnp.int32)[None, None, :]) % GROUP_SIZE
    chosen_tables = local_table[jnp.arange(block_count)[:, None], group_ids]
    local_ids = jnp.take_along_axis(chosen_tables, spot_index, axis=2)
    return (group_ids[:, :, None] * GROUP_SIZE + local_ids).reshape(TOKENS, TOP_K).astype(jnp.int32)


def draw_cache_latent(key, part):
    key_list = jax.random.split(jax.random.fold_in(key, 17), 1)
    values = jnp.clip(jax.random.normal(key_list[0], (TOKENS, CACHE, KV_RANK), jnp.float32), -6.0, 6.0)
    return values.astype(jnp.bfloat16)


def block_levels(key, dims, cuts, least, high):
    loudness = 1.0
    for axis_at, shards_of in cuts:
        steps = jax.random.uniform(jax.random.fold_in(jax.random.fold_in(key, 6), axis_at), (shards_of,), jnp.float32, least / len(cuts), high / len(cuts))
        loudness = loudness * jnp.repeat(jnp.exp(steps), dims[axis_at] // shards_of).reshape((-1,) + (1,) * (len(dims) - 1 - axis_at))
    return loudness


def scatter_about(rng, shape, deviation, limit, cuts=(), held_as=jnp.bfloat16):
    values = jax.random.normal(rng, shape, jnp.float32) * deviation
    if len(cuts) > 0:
        values = block_levels(rng, shape, cuts, -0.22, 0.18) * values
    return jnp.clip(values, min=-limit, max=limit).astype(held_as)


def setup_inputs(seed: int = 0) -> dict:
    arg_keys = jax.random.split(jax.random.key(seed), 21)
    return {
        "tokens": scatter_about(arg_keys[0], (TOKENS, D), 1.0, 6.0, ((0, 128),)),
        "cache_latent": draw_cache_latent(jax.random.fold_in(arg_keys[20], 71), 0),
        "cache_rope": scatter_about(arg_keys[2], (TOKENS, CACHE, ROPE_DIM), 1.0, 6.0, ((0, 128),)),
        "cache_lengths": draw_cache_lengths(jax.random.fold_in(arg_keys[20], 71), 0),
        "expert_ids": draw_expert_ids(jax.random.fold_in(arg_keys[20], 71), 0),
        "route_weight": jnp.clip(1.0 + 1.0 * jax.random.uniform(arg_keys[5], (TOKENS, TOP_K), jnp.float32) ** block_levels(arg_keys[5], (TOKENS, TOP_K), ((0, 128),), -0.2, 0.2), 1.0, 2.0),
        "attn_gain": jnp.clip(1.0 + 0.18 * jax.random.normal(arg_keys[6], (D,), jnp.float32), 0.1, 1.9),
        "q_gain": jnp.clip(1.0 + 0.18 * jax.random.normal(arg_keys[7], (Q_RANK,), jnp.float32), 0.1, 1.9),
        "kv_gain": jnp.clip(1.0 + 0.18 * jax.random.normal(arg_keys[8], (KV_RANK,), jnp.float32), 0.1, 1.9),
        "moe_gain": jnp.clip(1.0 + 0.18 * jax.random.normal(arg_keys[9], (D,), jnp.float32), 0.1, 1.9),
        "w_qdown": scatter_about(arg_keys[10], (D, Q_RANK), D ** -0.5, 0.125),
        "w_kvdown": scatter_about(arg_keys[11], (D, KV_RANK), D ** -0.5, 0.125),
        "w_krope": scatter_about(arg_keys[12], (D, ROPE_DIM), D ** -0.5, 0.125),
        "w_qup": scatter_about(arg_keys[13], (Q_RANK, HEADS * (NOPE_DIM + ROPE_DIM)), Q_RANK ** -0.5, 0.25),
        "w_kup": scatter_about(arg_keys[14], (KV_RANK, HEADS * NOPE_DIM), NOPE_DIM ** -0.5, 0.5),
        "w_vup": scatter_about(arg_keys[15], (KV_RANK, HEADS * VALUE_DIM), KV_RANK ** -0.5, 0.25),
        "w_out": scatter_about(arg_keys[16], (HEADS * VALUE_DIM, D), (HEADS * VALUE_DIM) ** -0.5, 0.1875),
        "expert_gate": scatter_about(arg_keys[17], (EXPERTS * 2, D, FF // 2), D ** -0.5, 0.125, ((0, 128),)),
        "expert_up": scatter_about(arg_keys[18], (EXPERTS * 2, D, FF // 2), D ** -0.5, 0.125, ((0, 128),)),
        "expert_down": scatter_about(arg_keys[19], (EXPERTS * 2, FF // 2, D), FF ** -0.5, 0.25, ((0, 128),)),
    }


EPS = 1e-06
THETA = 10000.0

def norm_gain(values, gain_vec):
    values = values.astype(jnp.float32)
    return values * lax.rsqrt(lax.optimization_barrier(jnp.mean(values * values, axis=-1, keepdims=True)) + EPS) * gain_vec.astype(jnp.float32)

def rotary_angles(lengths):
    half_width = ROPE_DIM // 2
    inverse = THETA ** (-jnp.arange(half_width, dtype=jnp.float32) / half_width)
    return lengths.astype(jnp.float32)[:, None] * inverse[None, :]

def rotate(values, angles):
    half_width = values.shape[-1] // 2
    first_half = values[..., :half_width]
    second = values[..., half_width:]
    cosine = jnp.cos(angles)
    sine_part = jnp.sin(angles)
    return jnp.concatenate([first_half * cosine - second * sine_part, second * cosine + first_half * sine_part], axis=-1)

def routed(moe_in, expert_ids, route_weight, expert_gate, expert_up, expert_down):
    row_count = moe_in.shape[0]
    most_rows = N_EP * CAPACITY
    padded = jnp.concatenate([moe_in, jnp.zeros((1, D), moe_in.dtype)], axis=0)

    def one_half(running, inputs):
        half_index, gate_half, up_half, down_half = inputs
        expert = half_index // 2
        match_mask = expert_ids == expert
        weight_sum = lax.optimization_barrier(jnp.sum(jnp.where(match_mask, route_weight, jnp.zeros_like(route_weight)), axis=1))
        chosen = jnp.nonzero(jnp.any(match_mask, axis=1), size=most_rows, fill_value=row_count)[0].astype(jnp.int32)
        slot_rows = padded[chosen]
        hidden = (jax.nn.silu(jnp.dot(slot_rows, gate_half, preferred_element_type=jnp.float32)) * jnp.dot(slot_rows, up_half, preferred_element_type=jnp.float32)).astype(jnp.bfloat16)
        part_out = jnp.dot(hidden, down_half, preferred_element_type=jnp.float32).astype(jnp.bfloat16).astype(jnp.float32)
        weight_pad = jnp.concatenate([weight_sum, jnp.zeros((1,), weight_sum.dtype)])[chosen]
        running = running.at[chosen].add(weight_pad[:, None] * part_out, mode='drop')
        return (running, None)
    halves = jnp.arange(expert_gate.shape[0], dtype=jnp.int32)
    running, _ = lax.scan(one_half, jnp.zeros((row_count, D), jnp.float32), (halves, expert_gate, expert_up, expert_down))
    return running

def reference(tokens, cache_latent, cache_rope, cache_lengths, expert_ids, route_weight, attn_gain, q_gain, kv_gain, moe_gain, w_qdown, w_kvdown, w_krope, w_qup, w_kup, w_vup, w_out, expert_gate, expert_up, expert_down):
    row_count = tokens.shape[0]
    score_scale = (NOPE_DIM + ROPE_DIM) ** (-0.5)
    normed = norm_gain(tokens, attn_gain).astype(jnp.bfloat16)
    q_low = norm_gain(jnp.dot(normed, w_qdown, preferred_element_type=jnp.float32), q_gain).astype(jnp.bfloat16)
    query_all = jnp.dot(q_low, w_qup, preferred_element_type=jnp.float32).reshape(row_count, HEADS, NOPE_DIM + ROPE_DIM)
    angles = rotary_angles(cache_lengths)
    q_nope = query_all[:, :, :NOPE_DIM].astype(jnp.bfloat16)
    q_rope = rotate(query_all[:, :, NOPE_DIM:], angles[:, None, :]).astype(jnp.bfloat16)
    new_latent = norm_gain(jnp.dot(normed, w_kvdown, preferred_element_type=jnp.float32), kv_gain).astype(jnp.bfloat16)
    new_rope_key = rotate(jnp.dot(normed, w_krope, preferred_element_type=jnp.float32), angles).astype(jnp.bfloat16)
    key_up = w_kup.reshape(KV_RANK, HEADS, NOPE_DIM).astype(jnp.float32)
    q_latent = jnp.einsum('thn,chn->thc', q_nope.astype(jnp.float32), key_up).astype(jnp.bfloat16)
    positions = jnp.arange(CACHE, dtype=jnp.int32)

    def one_sequence(inputs):
        q_lat, q_rot, cached, cached_rope, length, latent, rope_key = inputs
        past = (jnp.dot(q_lat, cached.T, preferred_element_type=jnp.float32) + jnp.dot(q_rot, cached_rope.T, preferred_element_type=jnp.float32)) * score_scale
        past = jnp.where(positions[None, :] < length, past, -jnp.inf)
        own_score = (jnp.dot(q_lat, latent, preferred_element_type=jnp.float32) + jnp.dot(q_rot, rope_key, preferred_element_type=jnp.float32)) * score_scale
        scores = jnp.concatenate([past, own_score[:, None]], axis=1)
        peak = lax.optimization_barrier(jnp.max(scores, axis=1, keepdims=True))
        raw_probs = jnp.exp(scores - peak)
        denom = lax.optimization_barrier(jnp.sum(raw_probs, axis=1, keepdims=True))
        probs = raw_probs.astype(jnp.bfloat16)
        summed = jnp.dot(probs[:, :CACHE], cached, preferred_element_type=jnp.float32) + probs[:, CACHE:].astype(jnp.float32) * latent.astype(jnp.float32)[None, :]
        return (summed / denom).astype(jnp.bfloat16)
    o_latent = lax.map(one_sequence, (q_latent, q_rope, cache_latent, cache_rope, cache_lengths, new_latent, new_rope_key))
    value_up = w_vup.reshape(KV_RANK, HEADS, VALUE_DIM).astype(jnp.float32)
    heads_out = jnp.einsum('thc,chv->thv', o_latent.astype(jnp.float32), value_up).astype(jnp.bfloat16)
    heads_out = heads_out.reshape(row_count, HEADS * VALUE_DIM)
    mixed_attn = (tokens.astype(jnp.float32) + jnp.dot(heads_out, w_out, preferred_element_type=jnp.float32)).astype(jnp.bfloat16)
    moe_in = norm_gain(mixed_attn, moe_gain).astype(jnp.bfloat16)
    moe_out = routed(moe_in, expert_ids, route_weight, expert_gate, expert_up, expert_down)
    mixed = mixed_attn.astype(jnp.float32) + moe_out
    return (mixed, new_latent, new_rope_key)
```

```python
import jax
import jax.numpy as jnp
import numpy as np
from jax import lax
from jax.experimental import pallas as pl
from jax.experimental.pallas import tpu as pltpu
from jax.sharding import PartitionSpec as P

HEADS = 8
KV_RANK = 512
NOPE_DIM = 128
ROPE_DIM = 64
TOP_K = 6
SEQ_DEV = 12
CACHE = 1024
D = 2048
CAPACITY = 3
SIDE = 4
CHIPS = 64
CHUNKS = 4
PER_CHUNK = CHIPS // CHUNKS
ROWS = PER_CHUNK * CAPACITY
SLOTS = CHIPS * CAPACITY
LANES = 128
TILES = D // LANES
PARTS = KV_RANK // LANES
EPS = 1e-06
THETA = 10000.0
F32 = jnp.float32
BF16 = jnp.bfloat16


def norm_gain(values, gain):
    return values * lax.rsqrt(jnp.mean(values * values, axis=-1, keepdims=True) + EPS) * gain


def dot(a, b):
    return jnp.dot(a, b, preferred_element_type=F32)


def dot_t(a, b):
    return lax.dot_general(a, b, (((1,), (1,)), ((), ())), preferred_element_type=F32)


def swap_halves(v):
    half = ROPE_DIM // 2
    return jnp.concatenate([v[:, half:], v[:, :half]], axis=1)


def chip_at(x, y, z):
    return z * (SIDE * SIDE) + y * SIDE + x


def wrap(v):
    return lax.rem(v + 2 * SIDE, SIDE)


def offset_of(p):
    chunk = p // PER_CHUNK
    dx = lax.rem(p, SIDE)
    dy = lax.rem(p // SIDE, SIDE)
    return dx, dy, wrap(chunk - dx - dy)


def kernel(
    len_s, weight_s, tok, ag, qg, kg, mg, ids, inv,
    cache, rope_t, qdown, kvdown, krope_t, qup, kup, vup, wout, gate, up, down,
    mixed_o, latent_o, key_o,
    cache_v, rope_v, qdown_v, kvdown_v, krope_v, qup_v, kup_v, vup_v, wout_v,
    gate_v, up_v, down_v,
    qlat, qrope, scores, olat, own_v, table_v, slot_v, table_s, slot_s,
    tile_f, attn_f, rows_b, send_b, recv_b, out_b, back_b, x_b,
    w_sem, cache_sem, rope_sem, e_sem, s_sem, x_send, x_recv,
    d_send, d_recv, r_send, r_recv,
):
    me = lax.axis_index("ep")
    core = lax.rem(me, 2)
    chip = me // 2
    mx = lax.rem(chip, SIDE)
    my = lax.rem(chip // SIDE, SIDE)
    mz = chip // (SIDE * SIDE)
    sibling = me + 1 - 2 * core

    def target(p, sign):
        dx, dy, dz = offset_of(p)
        there = chip_at(wrap(mx + sign * dx), wrap(my + sign * dy), wrap(mz + sign * dz))
        return there

    barrier = pltpu.get_barrier_semaphore()

    weights = [
        (qdown, qdown_v), (qup, qup_v), (kup, kup_v), (kvdown, kvdown_v), (krope_t, krope_v),
        (vup, vup_v), (wout, wout_v),
    ]
    w_copy = [
        pltpu.make_async_copy(src, dst, w_sem.at[i]) for i, (src, dst) in enumerate(weights)
    ]
    experts = [(gate, gate_v), (up, up_v), (down, down_v)]
    e_copy = [
        pltpu.make_async_copy(src.at[0], dst.at[0], e_sem.at[i])
        for i, (src, dst) in enumerate(experts)
    ]

    def cache_copies(t):
        return (
            pltpu.make_async_copy(cache.at[t], cache_v.at[t], cache_sem.at[t]),
            pltpu.make_async_copy(rope_t.at[t], rope_v.at[t], rope_sem.at[t]),
        )

    def start_cache(t):
        for c in cache_copies(t):
            c.start()

    for i in range(5):
        w_copy[i].start()
    for t in range(6):
        start_cache(t)

    def greet(p, carry):
        pl.semaphore_signal(
            barrier, inc=1, device_id=(target(p, 1) * 2 + core,),
            device_id_type=pl.DeviceIdType.MESH,
        )
        return carry

    lax.fori_loop(1, CHIPS, greet, 0)
    pl.semaphore_signal(
        barrier, inc=1, device_id=(sibling,), device_id_type=pl.DeviceIdType.MESH
    )

    ids_v = ids[...]
    table_v[...] = jnp.zeros((8, LANES), jnp.int32)
    slot_v[...] = jnp.zeros((8, LANES), jnp.int32)
    expert_iota = lax.broadcasted_iota(jnp.int32, (LANES, SEQ_DEV), 0)
    hits = jnp.zeros((LANES, SEQ_DEV), F32)
    for k in range(TOP_K):
        hits = jnp.where(expert_iota == ids_v[k : k + 1, :], 1.0, hits)
    before = jnp.where(
        lax.broadcasted_iota(jnp.int32, (SEQ_DEV, SEQ_DEV), 0)
        < lax.broadcasted_iota(jnp.int32, (SEQ_DEV, SEQ_DEV), 1),
        1.0,
        0.0,
    )
    rank = dot(hits.astype(BF16), before.astype(BF16))
    token_less = (
        lax.broadcasted_iota(jnp.int32, (8, SEQ_DEV), 1).astype(F32) - SEQ_DEV
    ).astype(BF16)
    row_iota = lax.broadcasted_iota(jnp.int32, (8, LANES), 0)
    table = jnp.zeros((8, LANES), F32)
    for s in range(CAPACITY):
        chosen = jnp.where(rank == float(s), hits, 0.0).astype(BF16)
        table = jnp.where(row_iota == s, dot_t(token_less, chosen) + SEQ_DEV, table)
    table_v[...] = jnp.clip(table.astype(jnp.int32), 0, SEQ_DEV)
    for k in range(TOP_K):
        e = ids_v[k : k + 1, :]
        own_rank = jnp.sum(jnp.where(expert_iota == e, rank, 0.0), axis=0, keepdims=True)
        dx = ((e & 3) - mx) & 3
        dy = (((e >> 2) & 3) - my) & 3
        dz = ((e >> 4) - mz) & 3
        place = ((dx + dy + dz) & 3) * PER_CHUNK + dx + SIDE * dy
        slot_v[k : k + 1, 0:SEQ_DEV] = place * CAPACITY + jnp.clip(
            own_rank.astype(jnp.int32), 0, CAPACITY - 1
        )
    table_copy = pltpu.make_async_copy(table_v, table_s, s_sem.at[0])
    slot_copy = pltpu.make_async_copy(slot_v, slot_s, s_sem.at[1])
    table_copy.start()
    slot_copy.start()

    row16 = lax.broadcasted_iota(jnp.int32, (16, ROPE_DIM), 0)
    length_col = jnp.zeros((16, ROPE_DIM), F32)
    for t in range(SEQ_DEV):
        length_col = jnp.where(row16 == t, len_s[t].astype(F32), length_col)
    angles = length_col * inv[0:1, 0:ROPE_DIM]
    cosine = jnp.cos(angles)[0:SEQ_DEV]
    first_half = lax.broadcasted_iota(jnp.int32, (16, ROPE_DIM), 1) < ROPE_DIM // 2
    sine = jnp.sin(angles)
    sine = jnp.where(first_half, -sine, sine)[0:SEQ_DEV]

    normed = norm_gain(tok[...].astype(F32), ag[...]).astype(BF16)
    w_copy[0].wait()
    q_low = norm_gain(dot(normed, qdown_v[...]), qg[...]).astype(BF16)
    w_copy[1].wait()
    query = dot(q_low, qup_v[...])
    w_copy[2].wait()
    head_width = NOPE_DIM + ROPE_DIM
    zeros64 = jnp.zeros((SEQ_DEV, LANES - ROPE_DIM), F32)
    for h in range(HEADS):
        nope = query[:, h * head_width : h * head_width + NOPE_DIM].astype(BF16)
        lat = dot_t(nope, kup_v[:, h * NOPE_DIM : (h + 1) * NOPE_DIM])
        for j in range(PARTS):
            qlat[j, pl.ds(h, SEQ_DEV, stride=HEADS), :] = lat[:, j * LANES : (j + 1) * LANES]
        rot = query[:, h * head_width + NOPE_DIM : (h + 1) * head_width]
        rot = rot * cosine + swap_halves(rot) * sine
        qrope[pl.ds(h, SEQ_DEV, stride=HEADS), :] = jnp.concatenate([rot, zeros64], axis=1)
    w_copy[3].wait()
    new_latent = norm_gain(dot(normed, kvdown_v[...]), kg[...]).astype(BF16)
    latent_o[...] = new_latent
    w_copy[4].wait()
    new_key = dot_t(normed, krope_v[...])
    new_key = (new_key * cosine + swap_halves(new_key) * sine).astype(BF16)
    key_o[...] = new_key
    own_all = jnp.concatenate([new_latent.astype(F32), new_key.astype(F32), zeros64], axis=1)
    for t in range(SEQ_DEV):
        own_v[t] = own_all[t : t + 1, :]

    scale = (NOPE_DIM + ROPE_DIM) ** (-0.5)
    position = lax.broadcasted_iota(jnp.int32, (HEADS, CACHE), 1)

    def rows_of(t):
        return pl.ds(pl.multiple_of(t * HEADS, HEADS), HEADS)

    def query_of(t):
        parts = [qlat[j, rows_of(t), :] for j in range(PARTS)]
        return jnp.concatenate(parts, axis=1).astype(BF16)

    def score_step(t):
        for c in cache_copies(t):
            c.wait()
        q = query_of(t)
        r = qrope[rows_of(t), :].astype(BF16)[:, :ROPE_DIM]
        s = (dot_t(q, cache_v[t]) + dot(r, rope_v[t])) * scale
        scores[rows_of(t), :] = jnp.where(position < len_s[t], s, -jnp.inf)

    def value_step(t):
        q = query_of(t).astype(F32)
        r = qrope[rows_of(t), :].astype(BF16).astype(F32)
        own_row = own_v[t]
        own_latent = own_row[:, 0:KV_RANK]
        own_key = own_row[:, KV_RANK : KV_RANK + LANES]
        own = (
            jnp.sum(q * own_latent, axis=1, keepdims=True)
            + jnp.sum(r * own_key, axis=1, keepdims=True)
        ) * scale
        s = scores[rows_of(t), :]
        peak = jnp.maximum(jnp.max(s, axis=1, keepdims=True), own)
        probs = jnp.exp(s - peak)
        own_prob = jnp.exp(own - peak)
        denom = jnp.sum(probs, axis=1, keepdims=True) + own_prob
        total = dot(probs.astype(BF16), cache_v[t])
        total = total + own_prob.astype(BF16).astype(F32) * own_latent
        total = total / denom
        for j in range(PARTS):
            olat[j, rows_of(t), :] = total[:, j * LANES : (j + 1) * LANES]

    score_step(0)
    score_step(1)

    def body(i, carry):
        start_cache(2 * i + 4)
        start_cache(2 * i + 5)
        score_step(2 * i)
        score_step(2 * i + 1)
        value_step(2 * i - 2)
        value_step(2 * i - 1)
        return carry

    lax.fori_loop(1, 3, body, 0)
    for c in e_copy:
        c.start()
    lax.fori_loop(3, 4, body, 0)
    w_copy[5].start()
    w_copy[6].start()

    def tail(i, carry):
        score_step(2 * i)
        score_step(2 * i + 1)
        value_step(2 * i - 2)
        value_step(2 * i - 1)
        return carry

    lax.fori_loop(4, 5, tail, 0)
    pl.semaphore_wait(barrier, CHIPS)
    swap = []
    for i, (_, dst) in enumerate(experts):
        e_copy[i].wait()
        swap.append(
            pltpu.make_async_remote_copy(
                src_ref=dst.at[0],
                dst_ref=dst.at[1],
                send_sem=x_send.at[i],
                recv_sem=x_recv.at[i],
                device_id=(sibling,),
                device_id_type=pl.DeviceIdType.MESH,
            )
        )
        swap[-1].start()
    lax.fori_loop(5, 6, tail, 0)
    value_step(10)
    value_step(11)

    w_copy[5].wait()
    heads = []
    for h in range(HEADS):
        parts = [olat[j, pl.ds(h, SEQ_DEV, stride=HEADS), :] for j in range(PARTS)]
        o = jnp.concatenate(parts, axis=1).astype(BF16)
        heads.append(dot(o, vup_v[:, h * LANES : (h + 1) * LANES]).astype(BF16))
    heads_out = jnp.concatenate(heads, axis=1)
    w_copy[6].wait()
    mixed_attn = (tok[...].astype(F32) + dot(heads_out, wout_v[...])).astype(BF16).astype(F32)
    moe_in = norm_gain(mixed_attn, mg[...])
    for j in range(TILES):
        cols = slice(j * LANES, (j + 1) * LANES)
        tile_f[pl.ds(j, SEQ_DEV, stride=TILES), :] = moe_in[:, cols]
        attn_f[pl.ds(j, SEQ_DEV, stride=TILES), :] = mixed_attn[:, cols]
    rows_b[0:SEQ_DEV] = (
        tile_f[0 : SEQ_DEV * TILES, :].reshape(SEQ_DEV, TILES, LANES).astype(BF16)
    )
    rows_b[SEQ_DEV] = jnp.zeros((TILES, LANES), BF16)

    table_copy.wait()
    slot_copy.wait()

    for s in range(CAPACITY):
        recv_b[s] = rows_b[table_s[s, chip]]

    def fill(p, carry):
        there = target(p, 1)
        for s in range(CAPACITY):
            send_b[p * CAPACITY + s] = rows_b[table_s[s, there]]
        return carry

    lax.fori_loop(1, CHIPS, fill, 0)

    def block(ref, p, count=1):
        return ref.at[pl.ds(p * CAPACITY, count * CAPACITY)]

    def dispatch(p):
        return pltpu.make_async_remote_copy(
            src_ref=block(send_b, p),
            dst_ref=block(recv_b, p),
            send_sem=d_send,
            recv_sem=d_recv.at[p // PER_CHUNK],
            device_id=(target(p, 1) * 2 + core,),
            device_id_type=pl.DeviceIdType.MESH,
        )

    def go_back(p):
        return pltpu.make_async_remote_copy(
            src_ref=block(out_b, p),
            dst_ref=block(back_b, p),
            send_sem=r_send,
            recv_sem=r_recv,
            device_id=(target(p, -1) * 2 + core,),
            device_id_type=pl.DeviceIdType.MESH,
        )

    def start_dispatch(p, carry):
        dispatch(p).start()
        return carry

    lax.fori_loop(1, CHIPS, start_dispatch, 0)
    for c in swap:
        c.wait()

    def expert_chunk(c):
        first = 1 if c == 0 else 0
        count = PER_CHUNK - first
        landed = block(recv_b, c * PER_CHUNK + first, count)
        pltpu.make_async_copy(landed, landed, d_recv.at[c]).wait()
        x = recv_b[c * ROWS : (c + 1) * ROWS].astype(F32)
        tile_f[...] = x.reshape(ROWS * TILES, LANES)
        for j in range(TILES):
            x_b[:, j * LANES : (j + 1) * LANES] = tile_f[
                pl.ds(j, ROWS, stride=TILES), :
            ].astype(BF16)
        xv = x_b[...]
        total = None
        for half in range(2):
            g = dot(xv, gate_v[half])
            u = dot(xv, up_v[half])
            hidden = (g / (1.0 + jnp.exp(-g)) * u).astype(BF16)
            part = dot(hidden, down_v[half])
            total = part if total is None else total + part
        for j in range(TILES):
            tile_f[pl.ds(j, ROWS, stride=TILES), :] = total[:, j * LANES : (j + 1) * LANES]
        out = tile_f[...].reshape(ROWS, TILES, LANES).astype(BF16)
        if c == 0:
            back_b[0:CAPACITY] = out[0:CAPACITY]
        out_b[c * ROWS : (c + 1) * ROWS] = out

        def start_back(p, carry):
            go_back(p).start()
            return carry

        lax.fori_loop(c * PER_CHUNK + first, (c + 1) * PER_CHUNK, start_back, 0)

    for c in range(CHUNKS):
        expert_chunk(c)

    others = block(back_b, 1, CHIPS - 1)
    pltpu.make_async_copy(others, others, r_recv).wait()
    for t in range(SEQ_DEV):
        acc = attn_f[t * TILES : (t + 1) * TILES, :]
        for k in range(TOP_K):
            acc = acc + weight_s[k, t] * back_b[slot_s[k, t]].astype(F32)
        mixed_o[t] = acc
    sent = block(send_b, 1, CHIPS - 1)
    pltpu.make_async_copy(sent, sent, d_send).wait()
    pltpu.make_async_copy(sent, sent, r_send).wait()


def shards(
    tokens, cache_latent, cache_rope, cache_lengths, expert_ids, route_weight,
    attn_gain, q_gain, kv_gain, moe_gain,
    w_qdown, w_kvdown, w_krope, w_qup, w_kup, w_vup, w_out,
    expert_gate, expert_up, expert_down,
):
    half = ROPE_DIM // 2
    inverse = np.float32(THETA) ** (-np.arange(half, dtype=np.float32) / np.float32(half))
    inverse = jnp.asarray(np.tile(inverse, LANES // half)[None, :].astype(np.float32))
    smem = pl.BlockSpec(memory_space=pltpu.SMEM)
    vmem = pl.BlockSpec(memory_space=pltpu.VMEM)
    anywhere = pl.BlockSpec(memory_space=pl.ANY)
    dma = pltpu.SemaphoreType.DMA
    scratch = [
        pltpu.VMEM((SEQ_DEV, CACHE, KV_RANK), BF16),
        pltpu.VMEM((SEQ_DEV, ROPE_DIM, CACHE), BF16),
        pltpu.VMEM((D, 512), BF16),
        pltpu.VMEM((D, KV_RANK), BF16),
        pltpu.VMEM((ROPE_DIM, D), BF16),
        pltpu.VMEM((512, 1536), BF16),
        pltpu.VMEM((KV_RANK, 1024), BF16),
        pltpu.VMEM((KV_RANK, 1024), BF16),
        pltpu.VMEM((1024, D), BF16),
        pltpu.VMEM((2, D, 256), BF16),
        pltpu.VMEM((2, D, 256), BF16),
        pltpu.VMEM((2, 256, D), BF16),
        pltpu.VMEM((PARTS, SEQ_DEV * HEADS, LANES), F32),
        pltpu.VMEM((SEQ_DEV * HEADS, LANES), F32),
        pltpu.VMEM((SEQ_DEV * HEADS, CACHE), F32),
        pltpu.VMEM((PARTS, SEQ_DEV * HEADS, LANES), F32),
        pltpu.VMEM((SEQ_DEV, 1, KV_RANK + LANES), F32),
        pltpu.VMEM((8, LANES), jnp.int32),
        pltpu.VMEM((8, LANES), jnp.int32),
        pltpu.SMEM((8, LANES), jnp.int32),
        pltpu.SMEM((8, LANES), jnp.int32),
        pltpu.VMEM((ROWS * TILES, LANES), F32),
        pltpu.VMEM((SEQ_DEV * TILES, LANES), F32),
        pltpu.VMEM((SEQ_DEV + 1, TILES, LANES), BF16),
        pltpu.VMEM((SLOTS, TILES, LANES), BF16),
        pltpu.VMEM((SLOTS, TILES, LANES), BF16),
        pltpu.VMEM((SLOTS, TILES, LANES), BF16),
        pltpu.VMEM((SLOTS, TILES, LANES), BF16),
        pltpu.VMEM((ROWS, D), BF16),
        dma((7,)), dma((SEQ_DEV,)), dma((SEQ_DEV,)), dma((3,)), dma((2,)),
        dma((3,)), dma((3,)),
        dma, dma((CHUNKS,)), dma, dma,
    ]
    mixed, latent, key = pl.pallas_call(
        kernel,
        out_shape=(
            jax.ShapeDtypeStruct((SEQ_DEV, TILES, LANES), F32),
            jax.ShapeDtypeStruct((SEQ_DEV, KV_RANK), BF16),
            jax.ShapeDtypeStruct((SEQ_DEV, ROPE_DIM), BF16),
        ),
        in_specs=[smem, smem] + [vmem] * 7 + [anywhere] * 12,
        out_specs=(vmem, vmem, vmem),
        scratch_shapes=scratch,
        compiler_params=pltpu.CompilerParams(
            collective_id=0, has_side_effects=True, vmem_limit_bytes=60 * 1024 * 1024
        ),
        name="layer",
    )(
        cache_lengths, route_weight.T, tokens,
        attn_gain[None, :], q_gain[None, :], kv_gain[None, :], moe_gain[None, :],
        expert_ids.T, inverse,
        cache_latent, jnp.swapaxes(cache_rope, 1, 2),
        w_qdown, w_kvdown, w_krope.T, w_qup, w_kup, w_vup, w_out,
        expert_gate, expert_up, expert_down,
    )
    return (mixed.reshape(SEQ_DEV, D), latent, key)


def solution(mesh):
    rows = P("ep", None)
    cube = P("ep", None, None)
    placed = (rows, cube, cube, P("ep"), rows, rows) + (P(),) * 11 + (cube, cube, cube)
    return jax.shard_map(
        shards,
        mesh=mesh,
        in_specs=placed,
        out_specs=(rows, rows, rows),
        check_vma=False,
    )
```

```python
import jax
import jax.numpy as jnp
import numpy as np
from jax import lax
from jax.experimental import pallas as pl
from jax.experimental.pallas import tpu as pltpu
from jax.sharding import PartitionSpec as P

HEADS = 8
KV_RANK = 512
NOPE_DIM = 128
ROPE_DIM = 64
TOP_K = 6
SEQ_DEV = 12
CACHE = 1024
D = 2048
CAPACITY = 3
SIDE = 4
CHIPS = 64
CHUNKS = 4
PER_CHUNK = CHIPS // CHUNKS
ROWS = PER_CHUNK * CAPACITY
SLOTS = CHIPS * CAPACITY
LANES = 128
TILES = D // LANES
FIRST = 9500
WINDOW = 9000
GROUP_END = (1, 1, 5, 5, 5, 5, 11, 11, 11, 11, 11, 11)
PARTS = KV_RANK // LANES
EPS = 1e-06
THETA = 10000.0
F32 = jnp.float32
BF16 = jnp.bfloat16


def norm_gain(values, gain):
    return values * lax.rsqrt(jnp.mean(values * values, axis=-1, keepdims=True) + EPS) * gain


def dot(a, b):
    return jnp.dot(a, b, preferred_element_type=F32)


def dot_t(a, b):
    return lax.dot_general(a, b, (((1,), (1,)), ((), ())), preferred_element_type=F32)


def swap_halves(v):
    half = ROPE_DIM // 2
    return jnp.concatenate([v[:, half:], v[:, :half]], axis=1)


def offset_of(p):
    dx = p % SIDE
    dy = p // SIDE % SIDE
    return dx, dy, (p // PER_CHUNK - dx - dy) % SIDE


def kernel(
    len_h, weight_h, tok_h, ag_h, qg_h, kg_h, mg_h, ids_h, inv_h,
    cache, rope_t, qdown, kvdown, krope_t, qup, kup, vup, wout, gate, up, down,
    mixed_o, latent_o, key_o,
    len_s, weight_s, tok, ag, qg, kg, mg, ids, inv,
    cache_v, rope_v, qdown_v, kvdown_v, krope_v, qup_v, kup_v, vup_v, wout_v,
    gate_v, up_v, down_v,
    qlat, qrope, olat, own_v, table_v, slot_v, table_s, slot_s,
    tile_f, attn_f, rows_b, send_b, recv_b, out_b, back_b, x_b,
    i_sem, w_sem, cache_sem, rope_sem, e_sem, s_sem, x_send, x_recv,
    d_send, d_recv, r_send, r_recv,
):
    me = lax.axis_index("ep")
    core = lax.rem(me, 2)
    chip = me // 2
    mx = lax.rem(chip, SIDE)
    my = lax.rem(chip // SIDE, SIDE)
    mz = chip // (SIDE * SIDE)
    sibling = me + 1 - 2 * core

    at_x = [lax.rem(mx + i, SIDE) for i in range(SIDE)]
    at_y = [lax.rem(my + i, SIDE) * SIDE for i in range(SIDE)]
    at_z = [lax.rem(mz + i, SIDE) * (SIDE * SIDE) for i in range(SIDE)]

    def target(p, sign=1):
        dx, dy, dz = offset_of(p)
        return at_x[sign * dx % SIDE] + at_y[sign * dy % SIDE] + at_z[sign * dz % SIDE]

    barrier = pltpu.get_barrier_semaphore()

    sizes = []
    queue = []
    began = []
    done = []

    def later(src, dst, sem, kib):
        queue.append(pltpu.make_async_copy(src, dst, sem))
        sizes.append(kib)
        return len(queue) - 1

    def halves(src, dst, sem, rows, kib):
        cut = rows // 2
        for i in range(2):
            last = later(
                src.at[i * cut : (i + 1) * cut], dst.at[i * cut : (i + 1) * cut],
                sem.at[i], kib // 2,
            )
        return last

    def cached(t):
        later(cache.at[t], cache_v.at[t], cache_sem.at[t], 1024)
        return later(rope_t.at[t], rope_v.at[t], rope_sem.at[t], 128)

    small = [
        (tok_h, tok), (ag_h, ag), (ids_h, ids), (inv_h, inv), (len_h, len_s),
        (qg_h, qg), (kg_h, kg), (mg_h, mg), (weight_h, weight_s),
    ]
    small_at = [later(src, dst, i_sem.at[i], 1) for i, (src, dst) in enumerate(small)][-1]
    qdown_at = halves(qdown, qdown_v, w_sem.at[0], D, 2048)
    qup_at = halves(qup, qup_v, w_sem.at[1], 512, 1536)
    kup_at = later(kup, kup_v, w_sem.at[2, 0], 1024)
    cache_at = [cached(t) for t in range(4)]
    kvdown_at = halves(kvdown, kvdown_v, w_sem.at[3], D, 2048)
    krope_at = later(krope_t, krope_v, w_sem.at[4, 0], 256)
    cache_at += [cached(t) for t in range(4, SEQ_DEV)]
    vup_at = later(vup, vup_v, w_sem.at[5, 0], 1024)
    wout_at = halves(wout, wout_v, w_sem.at[6], 1024, 4096)
    experts = [(gate, gate_v), (up, up_v), (down, down_v)]
    expert_at = [
        later(src.at[0], dst.at[0], e_sem.at[i], 1024) for i, (src, dst) in enumerate(experts)
    ][-1]

    def refill(window):
        while len(began) < len(queue) and (
            sum(sizes[len(done) : len(began) + 1]) <= window
        ):
            queue[len(began)].start(priority=int(len(began) > kup_at))
            began.append(True)

    def need(last, window=WINDOW):
        while len(done) <= last:
            queue[len(done)].wait()
            done.append(True)
            refill(window)

    refill(FIRST)

    def signal(sem, device):
        pl.semaphore_signal(
            sem, inc=1, device_id=(device,), device_id_type=pl.DeviceIdType.MESH
        )

    for p in range(1, CHIPS):
        signal(barrier, target(p) * 2 + core)
    signal(barrier, sibling)
    need(small_at, FIRST)

    ids_v = ids[...]
    table_v[...] = jnp.zeros((8, LANES), jnp.int32)
    slot_v[...] = jnp.zeros((8, LANES), jnp.int32)
    expert_iota = lax.broadcasted_iota(jnp.int32, (LANES, SEQ_DEV), 0)
    hits = jnp.zeros((LANES, SEQ_DEV), F32)
    for k in range(TOP_K):
        hits = jnp.where(expert_iota == ids_v[k : k + 1, :], 1.0, hits)
    before = jnp.where(
        lax.broadcasted_iota(jnp.int32, (SEQ_DEV, SEQ_DEV), 0)
        < lax.broadcasted_iota(jnp.int32, (SEQ_DEV, SEQ_DEV), 1),
        1.0,
        0.0,
    )
    rank = dot(hits.astype(BF16), before.astype(BF16))
    token_less = (
        lax.broadcasted_iota(jnp.int32, (8, SEQ_DEV), 1).astype(F32) - SEQ_DEV
    ).astype(BF16)
    row_iota = lax.broadcasted_iota(jnp.int32, (8, LANES), 0)
    table = jnp.zeros((8, LANES), F32)
    for s in range(CAPACITY):
        chosen = jnp.where(rank == float(s), hits, 0.0).astype(BF16)
        table = jnp.where(row_iota == s, dot_t(token_less, chosen) + SEQ_DEV, table)
    table_v[...] = jnp.clip(table.astype(jnp.int32), 0, SEQ_DEV)
    for k in range(TOP_K):
        e = ids_v[k : k + 1, :]
        own_rank = jnp.sum(jnp.where(expert_iota == e, rank, 0.0), axis=0, keepdims=True)
        dx = ((e & 3) - mx) & 3
        dy = (((e >> 2) & 3) - my) & 3
        dz = ((e >> 4) - mz) & 3
        place = ((dx + dy + dz) & 3) * PER_CHUNK + dx + SIDE * dy
        slot_v[k : k + 1, 0:SEQ_DEV] = place * CAPACITY + jnp.clip(
            own_rank.astype(jnp.int32), 0, CAPACITY - 1
        )
    table_copy = pltpu.make_async_copy(table_v, table_s, s_sem.at[0])
    slot_copy = pltpu.make_async_copy(slot_v, slot_s, s_sem.at[1])
    table_copy.start()
    slot_copy.start()

    row16 = lax.broadcasted_iota(jnp.int32, (16, ROPE_DIM), 0)
    length_col = jnp.zeros((16, ROPE_DIM), F32)
    for t in range(SEQ_DEV):
        length_col = jnp.where(row16 == t, len_s[t].astype(F32), length_col)
    angles = length_col * inv[0:1, 0:ROPE_DIM]
    cosine = jnp.cos(angles)[0:SEQ_DEV]
    first_half = lax.broadcasted_iota(jnp.int32, (16, ROPE_DIM), 1) < ROPE_DIM // 2
    sine = jnp.sin(angles)
    sine = jnp.where(first_half, -sine, sine)[0:SEQ_DEV]

    normed = norm_gain(tok[...].astype(F32), ag[...]).astype(BF16)
    need(qdown_at)
    q_low = norm_gain(dot(normed, qdown_v[...]), qg[...]).astype(BF16)
    need(qup_at)
    query = dot(q_low, qup_v[...])
    need(kup_at)
    head_width = NOPE_DIM + ROPE_DIM
    zeros64 = jnp.zeros((SEQ_DEV, LANES - ROPE_DIM), F32)
    for h in range(HEADS):
        nope = query[:, h * head_width : h * head_width + NOPE_DIM].astype(BF16)
        lat = dot_t(nope, kup_v[:, h * NOPE_DIM : (h + 1) * NOPE_DIM])
        for j in range(PARTS):
            qlat[j, pl.ds(h, SEQ_DEV, stride=HEADS), :] = lat[:, j * LANES : (j + 1) * LANES]
        rot = query[:, h * head_width + NOPE_DIM : (h + 1) * head_width]
        rot = rot * cosine + swap_halves(rot) * sine
        qrope[pl.ds(h, SEQ_DEV, stride=HEADS), :] = jnp.concatenate([rot, zeros64], axis=1)
    scale = (NOPE_DIM + ROPE_DIM) ** (-0.5)
    position = lax.broadcasted_iota(jnp.int32, (HEADS, CACHE), 1)

    def rows_of(t):
        return slice(t * HEADS, (t + 1) * HEADS)

    def query_of(t):
        parts = [qlat[j, rows_of(t), :] for j in range(PARTS)]
        return jnp.concatenate(parts, axis=1).astype(BF16)

    def score_step(t):
        need(cache_at[GROUP_END[t]])
        q = query_of(t)
        r = qrope[rows_of(t), :].astype(BF16)[:, :ROPE_DIM]
        s = (dot_t(q, cache_v[t]) + dot(r, rope_v[t])) * scale
        return jnp.where(position < len_s[t], s, -jnp.inf)

    def value_step(t, s):
        q = query_of(t).astype(F32)
        r = qrope[rows_of(t), :].astype(BF16).astype(F32)
        own_row = own_v[t]
        own_latent = own_row[:, 0:KV_RANK]
        own_key = own_row[:, KV_RANK : KV_RANK + LANES]
        own = (
            jnp.sum(q * own_latent, axis=1, keepdims=True)
            + jnp.sum(r * own_key, axis=1, keepdims=True)
        ) * scale
        peak = jnp.maximum(jnp.max(s, axis=1, keepdims=True), own)
        probs = jnp.exp(s - peak)
        own_prob = jnp.exp(own - peak)
        denom = jnp.sum(probs, axis=1, keepdims=True) + own_prob
        total = dot(probs.astype(BF16), cache_v[t])
        total = total + own_prob.astype(BF16).astype(F32) * own_latent
        total = total / denom
        for j in range(PARTS):
            olat[j, rows_of(t), :] = total[:, j * LANES : (j + 1) * LANES]

    held = (score_step(0), score_step(1))
    need(kvdown_at)
    new_latent = norm_gain(dot(normed, kvdown_v[...]), kg[...]).astype(BF16)
    latent_o[...] = new_latent
    need(krope_at)
    new_key = dot_t(normed, krope_v[...])
    new_key = (new_key * cosine + swap_halves(new_key) * sine).astype(BF16)
    key_o[...] = new_key
    own_all = jnp.concatenate([new_latent.astype(F32), new_key.astype(F32), zeros64], axis=1)
    for t in range(SEQ_DEV):
        own_v[t] = own_all[t : t + 1, :]
    for i in range(1, SEQ_DEV // 2):
        fresh = (score_step(2 * i), score_step(2 * i + 1))
        value_step(2 * i - 2, held[0])
        value_step(2 * i - 1, held[1])
        held = fresh
    value_step(10, held[0])
    value_step(11, held[1])

    need(vup_at)
    heads = []
    for h in range(HEADS):
        parts = [olat[j, pl.ds(h, SEQ_DEV, stride=HEADS), :] for j in range(PARTS)]
        o = jnp.concatenate(parts, axis=1).astype(BF16)
        heads.append(dot(o, vup_v[:, h * LANES : (h + 1) * LANES]).astype(BF16))
    heads_out = jnp.concatenate(heads, axis=1)
    need(wout_at)
    pl.semaphore_wait(barrier, CHIPS)
    need(expert_at)
    swap = [
        pltpu.make_async_remote_copy(
            src_ref=dst.at[0],
            dst_ref=dst.at[1],
            send_sem=x_send.at[i],
            recv_sem=x_recv.at[i],
            device_id=(sibling,),
            device_id_type=pl.DeviceIdType.MESH,
        )
        for i, (_, dst) in enumerate(experts)
    ]
    for c in swap:
        c.start()
    mixed_attn = (tok[...].astype(F32) + dot(heads_out, wout_v[...])).astype(BF16).astype(F32)
    moe_in = norm_gain(mixed_attn, mg[...])
    for j in range(TILES):
        cols = slice(j * LANES, (j + 1) * LANES)
        tile_f[pl.ds(j, SEQ_DEV, stride=TILES), :] = moe_in[:, cols]
        attn_f[pl.ds(j, SEQ_DEV, stride=TILES), :] = mixed_attn[:, cols]
    rows_b[0:SEQ_DEV] = (
        tile_f[0 : SEQ_DEV * TILES, :].reshape(SEQ_DEV, TILES, LANES).astype(BF16)
    )
    rows_b[SEQ_DEV] = jnp.zeros((TILES, LANES), BF16)

    table_copy.wait()
    slot_copy.wait()

    def block(ref, p, count=1):
        return ref.at[pl.ds(p * CAPACITY, count * CAPACITY)]

    def dispatch(p):
        return pltpu.make_async_remote_copy(
            src_ref=block(send_b, p),
            dst_ref=block(recv_b, p),
            send_sem=d_send,
            recv_sem=d_recv.at[p // PER_CHUNK],
            device_id=(target(p, 1) * 2 + core,),
            device_id_type=pl.DeviceIdType.MESH,
        )

    def go_back(p):
        return pltpu.make_async_remote_copy(
            src_ref=block(out_b, p),
            dst_ref=block(back_b, p),
            send_sem=r_send,
            recv_sem=r_recv,
            device_id=(target(p, -1) * 2 + core,),
            device_id_type=pl.DeviceIdType.MESH,
        )

    def fill(c):
        for p in range(c * PER_CHUNK, (c + 1) * PER_CHUNK):
            there = target(p, 1)
            to = send_b if p else recv_b
            for s in range(CAPACITY):
                to[p * CAPACITY + s] = rows_b[table_s[s, there]]

    def send(c):
        for p in range(max(1, c * PER_CHUNK), (c + 1) * PER_CHUNK):
            dispatch(p).start()

    fill(0)
    for c in range(CHUNKS):
        if c + 1 < CHUNKS:
            fill(c + 1)
        send(c)
    for c in swap:
        c.wait()

    def expert_chunk(c):
        first = 1 if c == 0 else 0
        count = PER_CHUNK - first
        landed = block(recv_b, c * PER_CHUNK + first, count)
        pltpu.make_async_copy(landed, landed, d_recv.at[c]).wait()
        x = recv_b[c * ROWS : (c + 1) * ROWS].astype(F32)
        tile_f[...] = x.reshape(ROWS * TILES, LANES)
        for j in range(TILES):
            x_b[:, j * LANES : (j + 1) * LANES] = tile_f[
                pl.ds(j, ROWS, stride=TILES), :
            ].astype(BF16)
        xv = x_b[...]
        total = None
        for half in range(2):
            g = dot(xv, gate_v[half])
            u = dot(xv, up_v[half])
            hidden = (g / (1.0 + jnp.exp(-g)) * u).astype(BF16)
            part = dot(hidden, down_v[half])
            total = part if total is None else total + part
        for j in range(TILES):
            tile_f[pl.ds(j, ROWS, stride=TILES), :] = total[:, j * LANES : (j + 1) * LANES]
        out = tile_f[...].reshape(ROWS, TILES, LANES).astype(BF16)
        if c == 0:
            back_b[0:CAPACITY] = out[0:CAPACITY]
        out_b[c * ROWS : (c + 1) * ROWS] = out

        for p in range(c * PER_CHUNK + first, (c + 1) * PER_CHUNK):
            go_back(p).start()

    for c in range(CHUNKS):
        expert_chunk(c)

    others = block(back_b, 1, CHIPS - 1)
    pltpu.make_async_copy(others, others, r_recv).wait()
    for t in range(SEQ_DEV):
        acc = attn_f[t * TILES : (t + 1) * TILES, :]
        for k in range(TOP_K):
            acc = acc + weight_s[k, t] * back_b[slot_s[k, t]].astype(F32)
        attn_f[t * TILES : (t + 1) * TILES, :] = acc
    for j in range(TILES):
        mixed_o[:, j * LANES : (j + 1) * LANES] = attn_f[pl.ds(j, SEQ_DEV, stride=TILES), :]
    sent = block(send_b, 1, CHIPS - 1)
    pltpu.make_async_copy(sent, sent, d_send).wait()
    pltpu.make_async_copy(sent, sent, r_send).wait()


def hand_over(mixed, latent, key, mixed_o, latent_o, key_o):
    mixed_o[...] = mixed[...]
    latent_o[...] = latent[...]
    key_o[...] = key[...]


def shards(
    tokens, cache_latent, cache_rope, cache_lengths, expert_ids, route_weight,
    attn_gain, q_gain, kv_gain, moe_gain,
    w_qdown, w_kvdown, w_krope, w_qup, w_kup, w_vup, w_out,
    expert_gate, expert_up, expert_down,
):
    half = ROPE_DIM // 2
    inverse = np.float32(THETA) ** (-np.arange(half, dtype=np.float32) / np.float32(half))
    inverse = jnp.asarray(np.tile(inverse, LANES // half)[None, :].astype(np.float32))
    vmem = pl.BlockSpec(memory_space=pltpu.VMEM)
    anywhere = pl.BlockSpec(memory_space=pl.ANY)
    dma = pltpu.SemaphoreType.DMA
    scratch = [
        pltpu.SMEM((SEQ_DEV,), jnp.int32),
        pltpu.SMEM((TOP_K, SEQ_DEV), F32),
        pltpu.VMEM((SEQ_DEV, D), BF16),
        pltpu.VMEM((1, D), F32),
        pltpu.VMEM((1, 512), F32),
        pltpu.VMEM((1, KV_RANK), F32),
        pltpu.VMEM((1, D), F32),
        pltpu.VMEM((TOP_K, SEQ_DEV), jnp.int32),
        pltpu.VMEM((1, LANES), F32),
        pltpu.VMEM((SEQ_DEV, CACHE, KV_RANK), BF16),
        pltpu.VMEM((SEQ_DEV, ROPE_DIM, CACHE), BF16),
        pltpu.VMEM((D, 512), BF16),
        pltpu.VMEM((D, KV_RANK), BF16),
        pltpu.VMEM((ROPE_DIM, D), BF16),
        pltpu.VMEM((512, 1536), BF16),
        pltpu.VMEM((KV_RANK, 1024), BF16),
        pltpu.VMEM((KV_RANK, 1024), BF16),
        pltpu.VMEM((1024, D), BF16),
        pltpu.VMEM((2, D, 256), BF16),
        pltpu.VMEM((2, D, 256), BF16),
        pltpu.VMEM((2, 256, D), BF16),
        pltpu.VMEM((PARTS, SEQ_DEV * HEADS, LANES), F32),
        pltpu.VMEM((SEQ_DEV * HEADS, LANES), F32),
        pltpu.VMEM((PARTS, SEQ_DEV * HEADS, LANES), F32),
        pltpu.VMEM((SEQ_DEV, 1, KV_RANK + LANES), F32),
        pltpu.VMEM((8, LANES), jnp.int32),
        pltpu.VMEM((8, LANES), jnp.int32),
        pltpu.SMEM((8, LANES), jnp.int32),
        pltpu.SMEM((8, LANES), jnp.int32),
        pltpu.VMEM((ROWS * TILES, LANES), F32),
        pltpu.VMEM((SEQ_DEV * TILES, LANES), F32),
        pltpu.VMEM((SEQ_DEV + 1, TILES, LANES), BF16),
        pltpu.VMEM((SLOTS, TILES, LANES), BF16),
        pltpu.VMEM((SLOTS, TILES, LANES), BF16),
        pltpu.VMEM((SLOTS, TILES, LANES), BF16),
        pltpu.VMEM((SLOTS, TILES, LANES), BF16),
        pltpu.VMEM((ROWS, D), BF16),
        dma((9,)), dma((7, 2)), dma((SEQ_DEV,)), dma((SEQ_DEV,)), dma((3,)), dma((2,)),
        dma((3,)), dma((3,)),
        dma, dma((CHUNKS,)), dma, dma,
    ]
    shapes = (
        jax.ShapeDtypeStruct((SEQ_DEV, D), F32),
        jax.ShapeDtypeStruct((SEQ_DEV, KV_RANK), BF16),
        jax.ShapeDtypeStruct((SEQ_DEV, ROPE_DIM), BF16),
    )
    done = pl.pallas_call(
        kernel,
        out_shape=shapes,
        in_specs=[anywhere] * 21,
        out_specs=(vmem, vmem, vmem),
        scratch_shapes=scratch,
        compiler_params=pltpu.CompilerParams(
            collective_id=0, has_side_effects=True, vmem_limit_bytes=60 * 1024 * 1024
        ),
        name="layer",
    )(
        cache_lengths, route_weight.T, tokens,
        attn_gain[None, :], q_gain[None, :], kv_gain[None, :], moe_gain[None, :],
        expert_ids.T, inverse,
        cache_latent, jnp.swapaxes(cache_rope, 1, 2),
        w_qdown, w_kvdown, w_krope.T, w_qup, w_kup, w_vup, w_out,
        expert_gate, expert_up, expert_down,
    )
    return pl.pallas_call(
        hand_over,
        out_shape=shapes,
        in_specs=[vmem] * 3,
        out_specs=(vmem, vmem, vmem),
        name="outputs",
    )(*done)


def solution(mesh):
    rows = P("ep", None)
    cube = P("ep", None, None)
    placed = (rows, cube, cube, P("ep"), rows, rows) + (P(),) * 11 + (cube, cube, cube)
    return jax.shard_map(
        shards,
        mesh=mesh,
        in_specs=placed,
        out_specs=(rows, rows, rows),
        check_vma=False,
    )
```

```python
import jax
import jax.numpy as jnp
import numpy as np
from jax import lax
from jax.experimental import pallas as pl
from jax.experimental.pallas import tpu as pltpu
from jax.sharding import PartitionSpec as P

HEADS = 8
KV_RANK = 512
NOPE_DIM = 128
ROPE_DIM = 64
TOP_K = 6
SEQ_DEV = 12
CACHE = 1024
D = 2048
CAPACITY = 3
SIDE = 4
CHIPS = 64
CHUNKS = 4
PER_CHUNK = CHIPS // CHUNKS
ROWS = PER_CHUNK * CAPACITY
SLOTS = CHIPS * CAPACITY
LANES = 128
TILES = D // LANES
FIRST = 9500
WINDOW = 9000
GROUP_END = (1, 1, 5, 5, 5, 5, 11, 11, 11, 11, 11, 11)
PARTS = KV_RANK // LANES
EPS = 1e-06
THETA = 10000.0
F32 = jnp.float32
BF16 = jnp.bfloat16


def norm_gain(values, gain):
    return values * lax.rsqrt(jnp.mean(values * values, axis=-1, keepdims=True) + EPS) * gain


def dot(a, b):
    return jnp.dot(a, b, preferred_element_type=F32)


def dot_t(a, b):
    return lax.dot_general(a, b, (((1,), (1,)), ((), ())), preferred_element_type=F32)


def swap_halves(v):
    half = ROPE_DIM // 2
    return jnp.concatenate([v[:, half:], v[:, :half]], axis=1)


def offset_of(p):
    dx = p % SIDE
    dy = p // SIDE % SIDE
    return dx, dy, (p // (SIDE * SIDE) - dx - dy) % SIDE


def kernel(
    len_h, weight_h, tok_h, ag_h, qg_h, kg_h, mg_h, ids_h, inv_h,
    cache, rope_t, qdown, kvdown, krope_t, qup, kup, vup, wout, gate, up, down,
    mixed_o, latent_o, key_o,
    len_s, weight_s, tok, ag, qg, kg, mg, ids, inv,
    cache_v, rope_v, qdown_v, kvdown_v, krope_v, qup_v, kup_v, vup_v, wout_v,
    gate_v, up_v, down_v,
    qlat, qrope, olat, own_v, table_v, slot_v, table_s, slot_s,
    tile_f, attn_f, rows_b, send_b, recv_b, out_b, back_b, x_b,
    i_sem, w_sem, cache_sem, rope_sem, e_sem, s_sem, x_send, x_recv,
    d_send, d_recv, r_send, r_recv,
):
    me = lax.axis_index("ep")
    core = lax.rem(me, 2)
    chip = me // 2
    mx = lax.rem(chip, SIDE)
    my = lax.rem(chip // SIDE, SIDE)
    mz = chip // (SIDE * SIDE)
    sibling = me + 1 - 2 * core

    at_x = [lax.rem(mx + i, SIDE) for i in range(SIDE)]
    at_y = [lax.rem(my + i, SIDE) * SIDE for i in range(SIDE)]
    at_z = [lax.rem(mz + i, SIDE) * (SIDE * SIDE) for i in range(SIDE)]

    def target(p, sign=1):
        dx, dy, dz = offset_of(p)
        return at_x[sign * dx % SIDE] + at_y[sign * dy % SIDE] + at_z[sign * dz % SIDE]

    barrier = pltpu.get_barrier_semaphore()

    sizes = []
    queue = []
    began = []
    done = []

    def later(src, dst, sem, kib):
        queue.append(pltpu.make_async_copy(src, dst, sem))
        sizes.append(kib)
        return len(queue) - 1

    def halves(src, dst, sem, rows, kib):
        cut = rows // 2
        for i in range(2):
            last = later(
                src.at[i * cut : (i + 1) * cut], dst.at[i * cut : (i + 1) * cut],
                sem.at[i], kib // 2,
            )
        return last

    def cached(t):
        later(cache.at[t], cache_v.at[t], cache_sem.at[t], 1024)
        return later(rope_t.at[t], rope_v.at[t], rope_sem.at[t], 128)

    small = [
        (tok_h, tok), (ag_h, ag), (ids_h, ids), (inv_h, inv), (len_h, len_s),
        (qg_h, qg), (kg_h, kg), (mg_h, mg), (weight_h, weight_s),
    ]
    small_at = [later(src, dst, i_sem.at[i], 1) for i, (src, dst) in enumerate(small)][-1]
    qdown_at = halves(qdown, qdown_v, w_sem.at[0], D, 2048)
    qup_at = halves(qup, qup_v, w_sem.at[1], 512, 1536)
    kup_at = later(kup, kup_v, w_sem.at[2, 0], 1024)
    cache_at = [cached(t) for t in range(4)]
    kvdown_at = halves(kvdown, kvdown_v, w_sem.at[3], D, 2048)
    krope_at = later(krope_t, krope_v, w_sem.at[4, 0], 256)
    cache_at += [cached(t) for t in range(4, SEQ_DEV)]
    vup_at = later(vup, vup_v, w_sem.at[5, 0], 1024)
    wout_at = halves(wout, wout_v, w_sem.at[6], 1024, 4096)
    experts = [(gate, gate_v), (up, up_v), (down, down_v)]
    expert_at = [
        later(src.at[0], dst.at[0], e_sem.at[i], 1024) for i, (src, dst) in enumerate(experts)
    ][-1]

    def refill(window):
        while len(began) < len(queue) and (
            sum(sizes[len(done) : len(began) + 1]) <= window
        ):
            queue[len(began)].start(priority=int(len(began) > kup_at))
            began.append(True)

    def need(last, window=WINDOW):
        while len(done) <= last:
            queue[len(done)].wait()
            done.append(True)
            refill(window)

    refill(FIRST)

    def signal(sem, device):
        pl.semaphore_signal(
            sem, inc=1, device_id=(device,), device_id_type=pl.DeviceIdType.MESH
        )

    for p in range(1, CHIPS):
        signal(barrier, target(p) * 2 + core)
    signal(barrier, sibling)
    need(small_at, FIRST)

    ids_v = ids[...]
    table_v[...] = jnp.zeros((8, LANES), jnp.int32)
    slot_v[...] = jnp.zeros((8, LANES), jnp.int32)
    expert_iota = lax.broadcasted_iota(jnp.int32, (LANES, SEQ_DEV), 0)
    hits = jnp.zeros((LANES, SEQ_DEV), F32)
    for k in range(TOP_K):
        hits = jnp.where(expert_iota == ids_v[k : k + 1, :], 1.0, hits)
    before = jnp.where(
        lax.broadcasted_iota(jnp.int32, (SEQ_DEV, SEQ_DEV), 0)
        < lax.broadcasted_iota(jnp.int32, (SEQ_DEV, SEQ_DEV), 1),
        1.0,
        0.0,
    )
    rank = dot(hits.astype(BF16), before.astype(BF16))
    token_less = (
        lax.broadcasted_iota(jnp.int32, (8, SEQ_DEV), 1).astype(F32) - SEQ_DEV
    ).astype(BF16)
    row_iota = lax.broadcasted_iota(jnp.int32, (8, LANES), 0)
    table = jnp.zeros((8, LANES), F32)
    for s in range(CAPACITY):
        chosen = jnp.where(rank == float(s), hits, 0.0).astype(BF16)
        table = jnp.where(row_iota == s, dot_t(token_less, chosen) + SEQ_DEV, table)
    table_v[...] = jnp.clip(table.astype(jnp.int32), 0, SEQ_DEV)
    for k in range(TOP_K):
        e = ids_v[k : k + 1, :]
        own_rank = jnp.sum(jnp.where(expert_iota == e, rank, 0.0), axis=0, keepdims=True)
        dx = ((e & 3) - mx) & 3
        dy = (((e >> 2) & 3) - my) & 3
        dz = ((e >> 4) - mz) & 3
        place = ((dx + dy + dz) & 3) * (SIDE * SIDE) + dx + SIDE * dy
        slot_v[k : k + 1, 0:SEQ_DEV] = place * CAPACITY + jnp.clip(
            own_rank.astype(jnp.int32), 0, CAPACITY - 1
        )
    table_copy = pltpu.make_async_copy(table_v, table_s, s_sem.at[0])
    slot_copy = pltpu.make_async_copy(slot_v, slot_s, s_sem.at[1])
    table_copy.start()
    slot_copy.start()

    row16 = lax.broadcasted_iota(jnp.int32, (16, ROPE_DIM), 0)
    length_col = jnp.zeros((16, ROPE_DIM), F32)
    for t in range(SEQ_DEV):
        length_col = jnp.where(row16 == t, len_s[t].astype(F32), length_col)
    angles = length_col * inv[0:1, 0:ROPE_DIM]
    cosine = jnp.cos(angles)[0:SEQ_DEV]
    first_half = lax.broadcasted_iota(jnp.int32, (16, ROPE_DIM), 1) < ROPE_DIM // 2
    sine = jnp.sin(angles)
    sine = jnp.where(first_half, -sine, sine)[0:SEQ_DEV]

    normed = norm_gain(tok[...].astype(F32), ag[...]).astype(BF16)
    need(qdown_at)
    q_low = norm_gain(dot(normed, qdown_v[...]), qg[...]).astype(BF16)
    need(qup_at)
    query = dot(q_low, qup_v[...])
    need(kup_at)
    head_width = NOPE_DIM + ROPE_DIM
    zeros64 = jnp.zeros((SEQ_DEV, LANES - ROPE_DIM), F32)
    for h in range(HEADS):
        nope = query[:, h * head_width : h * head_width + NOPE_DIM].astype(BF16)
        lat = dot_t(nope, kup_v[:, h * NOPE_DIM : (h + 1) * NOPE_DIM])
        for j in range(PARTS):
            qlat[j, pl.ds(h, SEQ_DEV, stride=HEADS), :] = lat[:, j * LANES : (j + 1) * LANES]
        rot = query[:, h * head_width + NOPE_DIM : (h + 1) * head_width]
        rot = rot * cosine + swap_halves(rot) * sine
        qrope[pl.ds(h, SEQ_DEV, stride=HEADS), :] = jnp.concatenate([rot, zeros64], axis=1)
    scale = (NOPE_DIM + ROPE_DIM) ** (-0.5)
    position = lax.broadcasted_iota(jnp.int32, (HEADS, CACHE), 1)

    def rows_of(t):
        return slice(t * HEADS, (t + 1) * HEADS)

    def query_of(t):
        parts = [qlat[j, rows_of(t), :] for j in range(PARTS)]
        return jnp.concatenate(parts, axis=1).astype(BF16)

    def score_step(t):
        need(cache_at[GROUP_END[t]])
        q = query_of(t)
        r = qrope[rows_of(t), :].astype(BF16)[:, :ROPE_DIM]
        s = (dot_t(q, cache_v[t]) + dot(r, rope_v[t])) * scale
        return jnp.where(position < len_s[t], s, -jnp.inf)

    def value_step(t, s):
        q = query_of(t).astype(F32)
        r = qrope[rows_of(t), :].astype(BF16).astype(F32)
        own_row = own_v[t]
        own_latent = own_row[:, 0:KV_RANK]
        own_key = own_row[:, KV_RANK : KV_RANK + LANES]
        own = (
            jnp.sum(q * own_latent, axis=1, keepdims=True)
            + jnp.sum(r * own_key, axis=1, keepdims=True)
        ) * scale
        peak = jnp.maximum(jnp.max(s, axis=1, keepdims=True), own)
        probs = jnp.exp(s - peak)
        own_prob = jnp.exp(own - peak)
        denom = jnp.sum(probs, axis=1, keepdims=True) + own_prob
        total = dot(probs.astype(BF16), cache_v[t])
        total = total + own_prob.astype(BF16).astype(F32) * own_latent
        total = total / denom
        for j in range(PARTS):
            olat[j, rows_of(t), :] = total[:, j * LANES : (j + 1) * LANES]

    held = (score_step(0), score_step(1))
    need(kvdown_at)
    new_latent = norm_gain(dot(normed, kvdown_v[...]), kg[...]).astype(BF16)
    latent_o[...] = new_latent
    need(krope_at)
    new_key = dot_t(normed, krope_v[...])
    new_key = (new_key * cosine + swap_halves(new_key) * sine).astype(BF16)
    key_o[...] = new_key
    own_all = jnp.concatenate([new_latent.astype(F32), new_key.astype(F32), zeros64], axis=1)
    for t in range(SEQ_DEV):
        own_v[t] = own_all[t : t + 1, :]
    for i in range(1, SEQ_DEV // 2):
        fresh = (score_step(2 * i), score_step(2 * i + 1))
        value_step(2 * i - 2, held[0])
        value_step(2 * i - 1, held[1])
        held = fresh
    value_step(10, held[0])
    value_step(11, held[1])

    need(vup_at)
    heads = []
    for h in range(HEADS):
        parts = [olat[j, pl.ds(h, SEQ_DEV, stride=HEADS), :] for j in range(PARTS)]
        o = jnp.concatenate(parts, axis=1).astype(BF16)
        heads.append(dot(o, vup_v[:, h * LANES : (h + 1) * LANES]).astype(BF16))
    heads_out = jnp.concatenate(heads, axis=1)
    need(wout_at)
    pl.semaphore_wait(barrier, CHIPS)
    need(expert_at)
    swap = [
        pltpu.make_async_remote_copy(
            src_ref=dst.at[0],
            dst_ref=dst.at[1],
            send_sem=x_send.at[i],
            recv_sem=x_recv.at[i],
            device_id=(sibling,),
            device_id_type=pl.DeviceIdType.MESH,
        )
        for i, (_, dst) in enumerate(experts)
    ]
    for c in swap:
        c.start()
    mixed_attn = (tok[...].astype(F32) + dot(heads_out, wout_v[...])).astype(BF16).astype(F32)
    moe_in = norm_gain(mixed_attn, mg[...])
    for j in range(TILES):
        cols = slice(j * LANES, (j + 1) * LANES)
        tile_f[pl.ds(j, SEQ_DEV, stride=TILES), :] = moe_in[:, cols]
        attn_f[pl.ds(j, SEQ_DEV, stride=TILES), :] = mixed_attn[:, cols]
    rows_b[0:SEQ_DEV] = (
        tile_f[0 : SEQ_DEV * TILES, :].reshape(SEQ_DEV, TILES, LANES).astype(BF16)
    )
    rows_b[SEQ_DEV] = jnp.zeros((TILES, LANES), BF16)

    table_copy.wait()
    slot_copy.wait()

    def block(ref, p, count=1):
        return ref.at[pl.ds(p * CAPACITY, count * CAPACITY)]

    def dispatch(p):
        return pltpu.make_async_remote_copy(
            src_ref=block(send_b, p),
            dst_ref=block(recv_b, p),
            send_sem=d_send,
            recv_sem=d_recv.at[p // PER_CHUNK],
            device_id=(target(p, 1) * 2 + core,),
            device_id_type=pl.DeviceIdType.MESH,
        )

    def go_back(p):
        return pltpu.make_async_remote_copy(
            src_ref=block(out_b, p),
            dst_ref=block(back_b, p),
            send_sem=r_send,
            recv_sem=r_recv,
            device_id=(target(p, -1) * 2 + core,),
            device_id_type=pl.DeviceIdType.MESH,
        )

    def fill(c):
        for p in range(c * PER_CHUNK, (c + 1) * PER_CHUNK):
            there = target(p, 1)
            to = send_b if p else recv_b
            for s in range(CAPACITY):
                to[p * CAPACITY + s] = rows_b[table_s[s, there]]

    def send(c):
        for p in range(max(1, c * PER_CHUNK), (c + 1) * PER_CHUNK):
            dispatch(p).start()

    fill(0)
    for c in range(CHUNKS):
        if c + 1 < CHUNKS:
            fill(c + 1)
        send(c)
    for c in swap:
        c.wait()

    def expert_chunk(c):
        first = 1 if c == 0 else 0
        count = PER_CHUNK - first
        landed = block(recv_b, c * PER_CHUNK + first, count)
        pltpu.make_async_copy(landed, landed, d_recv.at[c]).wait()
        x = recv_b[c * ROWS : (c + 1) * ROWS].astype(F32)
        tile_f[...] = x.reshape(ROWS * TILES, LANES)
        for j in range(TILES):
            x_b[:, j * LANES : (j + 1) * LANES] = tile_f[
                pl.ds(j, ROWS, stride=TILES), :
            ].astype(BF16)
        xv = x_b[...]
        total = None
        for half in range(2):
            g = dot(xv, gate_v[half])
            u = dot(xv, up_v[half])
            hidden = (g / (1.0 + jnp.exp(-g)) * u).astype(BF16)
            part = dot(hidden, down_v[half])
            total = part if total is None else total + part
        for j in range(TILES):
            tile_f[pl.ds(j, ROWS, stride=TILES), :] = total[:, j * LANES : (j + 1) * LANES]
        out = tile_f[...].reshape(ROWS, TILES, LANES).astype(BF16)
        if c == 0:
            back_b[0:CAPACITY] = out[0:CAPACITY]
        out_b[c * ROWS : (c + 1) * ROWS] = out

        for p in range(c * PER_CHUNK + first, (c + 1) * PER_CHUNK):
            go_back(p).start()

    for c in range(CHUNKS):
        expert_chunk(c)

    others = block(back_b, 1, CHIPS - 1)
    pltpu.make_async_copy(others, others, r_recv).wait()
    for t in range(SEQ_DEV):
        acc = attn_f[t * TILES : (t + 1) * TILES, :]
        for k in range(TOP_K):
            acc = acc + weight_s[k, t] * back_b[slot_s[k, t]].astype(F32)
        attn_f[t * TILES : (t + 1) * TILES, :] = acc
    for j in range(TILES):
        mixed_o[:, j * LANES : (j + 1) * LANES] = attn_f[pl.ds(j, SEQ_DEV, stride=TILES), :]
    sent = block(send_b, 1, CHIPS - 1)
    pltpu.make_async_copy(sent, sent, d_send).wait()
    pltpu.make_async_copy(sent, sent, r_send).wait()


def shards(
    tokens, cache_latent, cache_rope, cache_lengths, expert_ids, route_weight,
    attn_gain, q_gain, kv_gain, moe_gain,
    w_qdown, w_kvdown, w_krope, w_qup, w_kup, w_vup, w_out,
    expert_gate, expert_up, expert_down,
):
    half = ROPE_DIM // 2
    inverse = np.float32(THETA) ** (-np.arange(half, dtype=np.float32) / np.float32(half))
    inverse = jnp.asarray(np.tile(inverse, LANES // half)[None, :].astype(np.float32))
    vmem = pl.BlockSpec(memory_space=pltpu.VMEM)
    anywhere = pl.BlockSpec(memory_space=pl.ANY)
    dma = pltpu.SemaphoreType.DMA
    scratch = [
        pltpu.SMEM((SEQ_DEV,), jnp.int32),
        pltpu.SMEM((TOP_K, SEQ_DEV), F32),
        pltpu.VMEM((SEQ_DEV, D), BF16),
        pltpu.VMEM((1, D), F32),
        pltpu.VMEM((1, 512), F32),
        pltpu.VMEM((1, KV_RANK), F32),
        pltpu.VMEM((1, D), F32),
        pltpu.VMEM((TOP_K, SEQ_DEV), jnp.int32),
        pltpu.VMEM((1, LANES), F32),
        pltpu.VMEM((SEQ_DEV, CACHE, KV_RANK), BF16),
        pltpu.VMEM((SEQ_DEV, ROPE_DIM, CACHE), BF16),
        pltpu.VMEM((D, 512), BF16),
        pltpu.VMEM((D, KV_RANK), BF16),
        pltpu.VMEM((ROPE_DIM, D), BF16),
        pltpu.VMEM((512, 1536), BF16),
        pltpu.VMEM((KV_RANK, 1024), BF16),
        pltpu.VMEM((KV_RANK, 1024), BF16),
        pltpu.VMEM((1024, D), BF16),
        pltpu.VMEM((2, D, 256), BF16),
        pltpu.VMEM((2, D, 256), BF16),
        pltpu.VMEM((2, 256, D), BF16),
        pltpu.VMEM((PARTS, SEQ_DEV * HEADS, LANES), F32),
        pltpu.VMEM((SEQ_DEV * HEADS, LANES), F32),
        pltpu.VMEM((PARTS, SEQ_DEV * HEADS, LANES), F32),
        pltpu.VMEM((SEQ_DEV, 1, KV_RANK + LANES), F32),
        pltpu.VMEM((8, LANES), jnp.int32),
        pltpu.VMEM((8, LANES), jnp.int32),
        pltpu.SMEM((8, LANES), jnp.int32),
        pltpu.SMEM((8, LANES), jnp.int32),
        pltpu.VMEM((ROWS * TILES, LANES), F32),
        pltpu.VMEM((SEQ_DEV * TILES, LANES), F32),
        pltpu.VMEM((SEQ_DEV + 1, TILES, LANES), BF16),
        pltpu.VMEM((SLOTS, TILES, LANES), BF16),
        pltpu.VMEM((SLOTS, TILES, LANES), BF16),
        pltpu.VMEM((SLOTS, TILES, LANES), BF16),
        pltpu.VMEM((SLOTS, TILES, LANES), BF16),
        pltpu.VMEM((ROWS, D), BF16),
        dma((9,)), dma((7, 2)), dma((SEQ_DEV,)), dma((SEQ_DEV,)), dma((3,)), dma((2,)),
        dma((3,)), dma((3,)),
        dma, dma((CHUNKS,)), dma, dma,
    ]
    return pl.pallas_call(
        kernel,
        out_shape=(
            pltpu.VMEM((SEQ_DEV, D), F32),
            pltpu.VMEM((SEQ_DEV, KV_RANK), BF16),
            pltpu.VMEM((SEQ_DEV, ROPE_DIM), BF16),
        ),
        in_specs=[anywhere] * 21,
        out_specs=(vmem, vmem, vmem),
        scratch_shapes=scratch,
        compiler_params=pltpu.CompilerParams(
            collective_id=0, has_side_effects=True, vmem_limit_bytes=60 * 1024 * 1024
        ),
        name="layer",
    )(
        cache_lengths, route_weight.T, tokens,
        attn_gain[None, :], q_gain[None, :], kv_gain[None, :], moe_gain[None, :],
        expert_ids.T, inverse,
        cache_latent, jnp.swapaxes(cache_rope, 1, 2),
        w_qdown, w_kvdown, w_krope.T, w_qup, w_kup, w_vup, w_out,
        expert_gate, expert_up, expert_down,
    )


def solution(mesh):
    rows = P("ep", None)
    cube = P("ep", None, None)
    placed = (rows, cube, cube, P("ep"), rows, rows) + (P(),) * 11 + (cube, cube, cube)
    return jax.shard_map(
        shards,
        mesh=mesh,
        in_specs=placed,
        out_specs=(rows, rows, rows),
        check_vma=False,
    )
```

```python
import jax
import jax.numpy as jnp
import numpy as np
from jax import lax
from jax.experimental import pallas as pl
from jax.experimental.pallas import tpu as pltpu
from jax.sharding import PartitionSpec as P

HEADS = 8
KV_RANK = 512
NOPE_DIM = 128
ROPE_DIM = 64
TOP_K = 6
SEQ_DEV = 12
CACHE = 1024
D = 2048
CAPACITY = 3
SIDE = 4
CHIPS = 64
CHUNKS = 4
PER_CHUNK = CHIPS // CHUNKS
ROWS = PER_CHUNK * CAPACITY
SLOTS = CHIPS * CAPACITY
LANES = 128
TILES = D // LANES
FIRST = 9500
WINDOW = 9000
GROUP_END = (1, 1, 5, 5, 5, 5, 11, 11, 11, 11, 11, 11)
PARTS = KV_RANK // LANES
EPS = 1e-06
THETA = 10000.0
F32 = jnp.float32
BF16 = jnp.bfloat16


def norm_gain(values, gain):
    return values * lax.rsqrt(jnp.mean(values * values, axis=-1, keepdims=True) + EPS) * gain


def dot(a, b):
    return jnp.dot(a, b, preferred_element_type=F32)


def dot_t(a, b):
    return lax.dot_general(a, b, (((1,), (1,)), ((), ())), preferred_element_type=F32)


def swap_halves(v):
    half = ROPE_DIM // 2
    return jnp.concatenate([v[:, half:], v[:, :half]], axis=1)


def offset_of(p):
    dx = p % SIDE
    dy = p // SIDE % SIDE
    return dx, dy, (p // (SIDE * SIDE) - dx - dy) % SIDE


def kernel(
    len_h, weight_h, tok_h, ag_h, qg_h, kg_h, mg_h, ids_h, inv_h,
    cache, rope_t, qdown, kvdown, krope_t, qup, kup, vup, wout, gate, up, down,
    mixed_o, latent_o, key_o,
    len_s, weight_s, tok, ag, qg, kg, mg, ids, inv,
    cache_v, rope_v, qdown_v, kvdown_v, krope_v, qup_v, kup_v, vup_v, wout_v,
    gate_v, up_v, down_v,
    qlat, qrope, olat, own_v, table_v, slot_v, table_s, slot_s,
    tile_f, attn_f, rows_b, send_b, recv_b, out_b, back_b, x_b,
    i_sem, w_sem, cache_sem, rope_sem, e_sem, s_sem, x_send, x_recv,
    d_send, d_recv, r_send, r_recv,
):
    me = lax.axis_index("ep")
    core = lax.rem(me, 2)
    chip = me // 2
    mx = lax.rem(chip, SIDE)
    my = lax.rem(chip // SIDE, SIDE)
    mz = chip // (SIDE * SIDE)
    sibling = me + 1 - 2 * core

    at_x = [lax.rem(mx + i, SIDE) for i in range(SIDE)]
    at_y = [lax.rem(my + i, SIDE) * SIDE for i in range(SIDE)]
    at_z = [lax.rem(mz + i, SIDE) * (SIDE * SIDE) for i in range(SIDE)]

    def target(p, sign=1):
        dx, dy, dz = offset_of(p)
        return at_x[sign * dx % SIDE] + at_y[sign * dy % SIDE] + at_z[sign * dz % SIDE]

    barrier = pltpu.get_barrier_semaphore()

    sizes = []
    queue = []
    began = []
    done = []

    def later(src, dst, sem, kib):
        queue.append(pltpu.make_async_copy(src, dst, sem))
        sizes.append(kib)
        return len(queue) - 1

    def halves(src, dst, sem, rows, kib):
        cut = rows // 2
        for i in range(2):
            last = later(
                src.at[i * cut : (i + 1) * cut], dst.at[i * cut : (i + 1) * cut],
                sem.at[i], kib // 2,
            )
        return last

    def cached(t):
        later(cache.at[t], cache_v.at[t], cache_sem.at[t], 1024)
        return later(rope_t.at[t], rope_v.at[t], rope_sem.at[t], 128)

    small = [
        (tok_h, tok), (ag_h, ag), (ids_h, ids), (inv_h, inv), (len_h, len_s),
        (qg_h, qg), (kg_h, kg), (mg_h, mg), (weight_h, weight_s),
    ]
    small_at = [later(src, dst, i_sem.at[i], 1) for i, (src, dst) in enumerate(small)][-1]
    qdown_at = halves(qdown, qdown_v, w_sem.at[0], D, 2048)
    qup_at = halves(qup, qup_v, w_sem.at[1], 512, 1536)
    kup_at = later(kup, kup_v, w_sem.at[2, 0], 1024)
    cache_at = [cached(t) for t in range(4)]
    kvdown_at = halves(kvdown, kvdown_v, w_sem.at[3], D, 2048)
    krope_at = later(krope_t, krope_v, w_sem.at[4, 0], 256)
    cache_at += [cached(t) for t in range(4, SEQ_DEV)]
    vup_at = later(vup, vup_v, w_sem.at[5, 0], 1024)
    wout_at = halves(wout, wout_v, w_sem.at[6], 1024, 4096)
    experts = [(gate, gate_v), (up, up_v), (down, down_v)]
    expert_at = [
        later(src.at[0], dst.at[0], e_sem.at[i], 1024) for i, (src, dst) in enumerate(experts)
    ][-1]

    def refill(window):
        while len(began) < len(queue) and (
            sum(sizes[len(done) : len(began) + 1]) <= window
        ):
            queue[len(began)].start(priority=int(len(began) > kup_at))
            began.append(True)

    def need(last, window=WINDOW):
        while len(done) <= last:
            queue[len(done)].wait()
            done.append(True)
            refill(window)

    refill(FIRST)

    def signal(sem, device):
        pl.semaphore_signal(
            sem, inc=1, device_id=(device,), device_id_type=pl.DeviceIdType.MESH
        )

    for p in range(1, CHIPS):
        signal(barrier, target(p) * 2 + core)
    signal(barrier, sibling)
    need(small_at, FIRST)

    ids_v = ids[...]
    table_v[...] = jnp.zeros((8, LANES), jnp.int32)
    slot_v[...] = jnp.zeros((8, LANES), jnp.int32)
    expert_iota = lax.broadcasted_iota(jnp.int32, (LANES, SEQ_DEV), 0)
    hits = jnp.zeros((LANES, SEQ_DEV), F32)
    for k in range(TOP_K):
        hits = jnp.where(expert_iota == ids_v[k : k + 1, :], 1.0, hits)
    before = jnp.where(
        lax.broadcasted_iota(jnp.int32, (SEQ_DEV, SEQ_DEV), 0)
        < lax.broadcasted_iota(jnp.int32, (SEQ_DEV, SEQ_DEV), 1),
        1.0,
        0.0,
    )
    rank = dot(hits.astype(BF16), before.astype(BF16))
    token_less = (
        lax.broadcasted_iota(jnp.int32, (8, SEQ_DEV), 1).astype(F32) - SEQ_DEV
    ).astype(BF16)
    row_iota = lax.broadcasted_iota(jnp.int32, (8, LANES), 0)
    table = jnp.zeros((8, LANES), F32)
    for s in range(CAPACITY):
        chosen = jnp.where(rank == float(s), hits, 0.0).astype(BF16)
        table = jnp.where(row_iota == s, dot_t(token_less, chosen) + SEQ_DEV, table)
    table_v[...] = jnp.clip(table.astype(jnp.int32), 0, SEQ_DEV)
    for k in range(TOP_K):
        e = ids_v[k : k + 1, :]
        own_rank = jnp.sum(jnp.where(expert_iota == e, rank, 0.0), axis=0, keepdims=True)
        dx = ((e & 3) - mx) & 3
        dy = (((e >> 2) & 3) - my) & 3
        dz = ((e >> 4) - mz) & 3
        place = ((dx + dy + dz) & 3) * (SIDE * SIDE) + dx + SIDE * dy
        slot_v[k : k + 1, 0:SEQ_DEV] = place * CAPACITY + jnp.clip(
            own_rank.astype(jnp.int32), 0, CAPACITY - 1
        )
    table_copy = pltpu.make_async_copy(table_v, table_s, s_sem.at[0])
    slot_copy = pltpu.make_async_copy(slot_v, slot_s, s_sem.at[1])
    table_copy.start()
    slot_copy.start()

    row16 = lax.broadcasted_iota(jnp.int32, (16, ROPE_DIM), 0)
    length_col = jnp.zeros((16, ROPE_DIM), F32)
    for t in range(SEQ_DEV):
        length_col = jnp.where(row16 == t, len_s[t].astype(F32), length_col)
    angles = length_col * inv[0:1, 0:ROPE_DIM]
    cosine = jnp.cos(angles)[0:SEQ_DEV]
    first_half = lax.broadcasted_iota(jnp.int32, (16, ROPE_DIM), 1) < ROPE_DIM // 2
    sine = jnp.sin(angles)
    sine = jnp.where(first_half, -sine, sine)[0:SEQ_DEV]

    normed = norm_gain(tok[...].astype(F32), ag[...]).astype(BF16)
    need(qdown_at)
    q_low = norm_gain(dot(normed, qdown_v[...]), qg[...]).astype(BF16)
    need(qup_at)
    query = dot(q_low, qup_v[...])
    need(kup_at)
    head_width = NOPE_DIM + ROPE_DIM
    zeros64 = jnp.zeros((SEQ_DEV, LANES - ROPE_DIM), F32)
    for h in range(HEADS):
        nope = query[:, h * head_width : h * head_width + NOPE_DIM].astype(BF16)
        lat = dot_t(nope, kup_v[:, h * NOPE_DIM : (h + 1) * NOPE_DIM])
        for j in range(PARTS):
            qlat[j, pl.ds(h, SEQ_DEV, stride=HEADS), :] = lat[:, j * LANES : (j + 1) * LANES]
        rot = query[:, h * head_width + NOPE_DIM : (h + 1) * head_width]
        rot = rot * cosine + swap_halves(rot) * sine
        qrope[pl.ds(h, SEQ_DEV, stride=HEADS), :] = jnp.concatenate([rot, zeros64], axis=1)
    scale = (NOPE_DIM + ROPE_DIM) ** (-0.5)
    position = lax.broadcasted_iota(jnp.int32, (HEADS, CACHE), 1)

    def rows_of(t):
        return slice(t * HEADS, (t + 1) * HEADS)

    def query_of(t):
        parts = [qlat[j, rows_of(t), :] for j in range(PARTS)]
        return jnp.concatenate(parts, axis=1).astype(BF16)

    def score_step(t):
        need(cache_at[GROUP_END[t]])
        q = query_of(t)
        r = qrope[rows_of(t), :].astype(BF16)[:, :ROPE_DIM]
        s = (dot_t(q, cache_v[t]) + dot(r, rope_v[t])) * scale
        return jnp.where(position < len_s[t], s, -jnp.inf)

    def value_step(t, s):
        q = query_of(t).astype(F32)
        r = qrope[rows_of(t), :].astype(BF16).astype(F32)
        own_row = own_v[t]
        own_latent = own_row[:, 0:KV_RANK]
        own_key = own_row[:, KV_RANK : KV_RANK + LANES]
        own = (
            jnp.sum(q * own_latent, axis=1, keepdims=True)
            + jnp.sum(r * own_key, axis=1, keepdims=True)
        ) * scale
        peak = jnp.maximum(jnp.max(s, axis=1, keepdims=True), own)
        probs = jnp.exp(s - peak)
        own_prob = jnp.exp(own - peak)
        denom = jnp.sum(probs, axis=1, keepdims=True) + own_prob
        total = dot(probs.astype(BF16), cache_v[t])
        total = total + own_prob.astype(BF16).astype(F32) * own_latent
        total = total / denom
        for j in range(PARTS):
            olat[j, rows_of(t), :] = total[:, j * LANES : (j + 1) * LANES]

    held = (score_step(0), score_step(1))
    need(kvdown_at)
    new_latent = norm_gain(dot(normed, kvdown_v[...]), kg[...]).astype(BF16)
    latent_o[...] = new_latent
    need(krope_at)
    new_key = dot_t(normed, krope_v[...])
    new_key = (new_key * cosine + swap_halves(new_key) * sine).astype(BF16)
    key_o[...] = new_key
    own_all = jnp.concatenate([new_latent.astype(F32), new_key.astype(F32), zeros64], axis=1)
    for t in range(SEQ_DEV):
        own_v[t] = own_all[t : t + 1, :]
    for i in range(1, SEQ_DEV // 2):
        fresh = (score_step(2 * i), score_step(2 * i + 1))
        value_step(2 * i - 2, held[0])
        value_step(2 * i - 1, held[1])
        held = fresh
    value_step(10, held[0])
    value_step(11, held[1])

    need(vup_at)
    heads = []
    for h in range(HEADS):
        parts = [olat[j, pl.ds(h, SEQ_DEV, stride=HEADS), :] for j in range(PARTS)]
        o = jnp.concatenate(parts, axis=1).astype(BF16)
        heads.append(dot(o, vup_v[:, h * LANES : (h + 1) * LANES]).astype(BF16))
    heads_out = jnp.concatenate(heads, axis=1)
    need(wout_at)
    pl.semaphore_wait(barrier, CHIPS)
    need(expert_at)
    swap = [
        pltpu.make_async_remote_copy(
            src_ref=dst.at[0],
            dst_ref=dst.at[1],
            send_sem=x_send.at[i],
            recv_sem=x_recv.at[i],
            device_id=(sibling,),
            device_id_type=pl.DeviceIdType.MESH,
        )
        for i, (_, dst) in enumerate(experts)
    ]
    for c in swap:
        c.start()
    mixed_attn = (tok[...].astype(F32) + dot(heads_out, wout_v[...])).astype(BF16).astype(F32)
    moe_in = norm_gain(mixed_attn, mg[...])
    for j in range(TILES):
        cols = slice(j * LANES, (j + 1) * LANES)
        tile_f[pl.ds(j, SEQ_DEV, stride=TILES), :] = moe_in[:, cols]
        attn_f[pl.ds(j, SEQ_DEV, stride=TILES), :] = mixed_attn[:, cols]
    rows_b[0:SEQ_DEV] = (
        tile_f[0 : SEQ_DEV * TILES, :].reshape(SEQ_DEV, TILES, LANES).astype(BF16)
    )
    rows_b[SEQ_DEV] = jnp.zeros((TILES, LANES), BF16)

    table_copy.wait()
    slot_copy.wait()

    def block(ref, p, count=1):
        return ref.at[pl.ds(p * CAPACITY, count * CAPACITY)]

    def dispatch(p):
        return pltpu.make_async_remote_copy(
            src_ref=block(send_b, p),
            dst_ref=block(recv_b, p),
            send_sem=d_send,
            recv_sem=d_recv.at[p // PER_CHUNK],
            device_id=(target(p, 1) * 2 + core,),
            device_id_type=pl.DeviceIdType.MESH,
        )

    def go_back(p):
        return pltpu.make_async_remote_copy(
            src_ref=block(out_b, p),
            dst_ref=block(back_b, p),
            send_sem=r_send,
            recv_sem=r_recv,
            device_id=(target(p, -1) * 2 + core,),
            device_id_type=pl.DeviceIdType.MESH,
        )

    def fill(c):
        for p in range(c * PER_CHUNK, (c + 1) * PER_CHUNK):
            there = target(p, 1)
            to = send_b if p else recv_b
            for s in range(CAPACITY):
                to[p * CAPACITY + s] = rows_b[table_s[s, there]]

    def send(c):
        for p in range(max(1, c * PER_CHUNK), (c + 1) * PER_CHUNK):
            dispatch(p).start()

    fill(0)
    for c in range(CHUNKS):
        if c + 1 < CHUNKS:
            fill(c + 1)
        send(c)
    for c in swap:
        c.wait()

    def expert_chunk(c):
        first = 1 if c == 0 else 0
        count = PER_CHUNK - first
        landed = block(recv_b, c * PER_CHUNK + first, count)
        pltpu.make_async_copy(landed, landed, d_recv.at[c]).wait()
        x = recv_b[c * ROWS : (c + 1) * ROWS].astype(F32)
        tile_f[...] = x.reshape(ROWS * TILES, LANES)
        for j in range(TILES):
            x_b[:, j * LANES : (j + 1) * LANES] = tile_f[
                pl.ds(j, ROWS, stride=TILES), :
            ].astype(BF16)
        xv = x_b[...]
        total = None
        for half in range(2):
            g = dot(xv, gate_v[half])
            u = dot(xv, up_v[half])
            hidden = (g / (1.0 + jnp.exp(-g)) * u).astype(BF16)
            part = dot(hidden, down_v[half])
            total = part if total is None else total + part
        for j in range(TILES):
            tile_f[pl.ds(j, ROWS, stride=TILES), :] = total[:, j * LANES : (j + 1) * LANES]
        out = tile_f[...].reshape(ROWS, TILES, LANES).astype(BF16)
        if c == 0:
            back_b[0:CAPACITY] = out[0:CAPACITY]
        out_b[c * ROWS : (c + 1) * ROWS] = out

        for p in range(c * PER_CHUNK + first, (c + 1) * PER_CHUNK):
            go_back(p).start()

    for c in range(CHUNKS):
        expert_chunk(c)

    others = block(back_b, 1, CHIPS - 1)
    pltpu.make_async_copy(others, others, r_recv).wait()
    for t in range(SEQ_DEV):
        acc = attn_f[t * TILES : (t + 1) * TILES, :]
        for k in range(TOP_K):
            acc = acc + weight_s[k, t] * back_b[slot_s[k, t]].astype(F32)
        attn_f[t * TILES : (t + 1) * TILES, :] = acc
    for j in range(TILES):
        mixed_o[:, j * LANES : (j + 1) * LANES] = attn_f[pl.ds(j, SEQ_DEV, stride=TILES), :]
    sent = block(send_b, 1, CHIPS - 1)
    pltpu.make_async_copy(sent, sent, d_send).wait()
    pltpu.make_async_copy(sent, sent, r_send).wait()


def shards(
    tokens, cache_latent, cache_rope, cache_lengths, expert_ids, route_weight,
    attn_gain, q_gain, kv_gain, moe_gain,
    w_qdown, w_kvdown, w_krope, w_qup, w_kup, w_vup, w_out,
    expert_gate, expert_up, expert_down,
):
    half = ROPE_DIM // 2
    inverse = np.float32(THETA) ** (-np.arange(half, dtype=np.float32) / np.float32(half))
    inverse = jnp.asarray(np.tile(inverse, LANES // half)[None, :].astype(np.float32))
    vmem = pl.BlockSpec(memory_space=pltpu.VMEM)
    anywhere = pl.BlockSpec(memory_space=pl.ANY)
    dma = pltpu.SemaphoreType.DMA
    scratch = [
        pltpu.SMEM((SEQ_DEV,), jnp.int32),
        pltpu.SMEM((TOP_K, SEQ_DEV), F32),
        pltpu.VMEM((SEQ_DEV, D), BF16),
        pltpu.VMEM((1, D), F32),
        pltpu.VMEM((1, 512), F32),
        pltpu.VMEM((1, KV_RANK), F32),
        pltpu.VMEM((1, D), F32),
        pltpu.VMEM((TOP_K, SEQ_DEV), jnp.int32),
        pltpu.VMEM((1, LANES), F32),
        pltpu.VMEM((SEQ_DEV, CACHE, KV_RANK), BF16),
        pltpu.VMEM((SEQ_DEV, ROPE_DIM, CACHE), BF16),
        pltpu.VMEM((D, 512), BF16),
        pltpu.VMEM((D, KV_RANK), BF16),
        pltpu.VMEM((ROPE_DIM, D), BF16),
        pltpu.VMEM((512, 1536), BF16),
        pltpu.VMEM((KV_RANK, 1024), BF16),
        pltpu.VMEM((KV_RANK, 1024), BF16),
        pltpu.VMEM((1024, D), BF16),
        pltpu.VMEM((2, D, 256), BF16),
        pltpu.VMEM((2, D, 256), BF16),
        pltpu.VMEM((2, 256, D), BF16),
        pltpu.VMEM((PARTS, 16 * HEADS, LANES), F32),
        pltpu.VMEM((16 * HEADS, LANES), F32),
        pltpu.VMEM((PARTS, 16 * HEADS, LANES), F32),
        pltpu.VMEM((SEQ_DEV + 8, 1, KV_RANK + LANES), F32),
        pltpu.VMEM((8, LANES), jnp.int32),
        pltpu.VMEM((8, LANES), jnp.int32),
        pltpu.SMEM((8, LANES), jnp.int32),
        pltpu.SMEM((8, LANES), jnp.int32),
        pltpu.VMEM((ROWS * TILES, LANES), F32),
        pltpu.VMEM((16 * TILES, LANES), F32),
        pltpu.VMEM((SEQ_DEV + 1, TILES, LANES), BF16),
        pltpu.VMEM((SLOTS, TILES, LANES), BF16),
        pltpu.VMEM((SLOTS, TILES, LANES), BF16),
        pltpu.VMEM((SLOTS, TILES, LANES), BF16),
        pltpu.VMEM((SLOTS, TILES, LANES), BF16),
        pltpu.VMEM((ROWS, D), BF16),
        dma((9,)), dma((7, 2)), dma((SEQ_DEV,)), dma((SEQ_DEV,)), dma((3,)), dma((2,)),
        dma((3,)), dma((3,)),
        dma, dma((CHUNKS,)), dma, dma,
    ]
    return pl.pallas_call(
        kernel,
        out_shape=(
            pltpu.VMEM((SEQ_DEV, D), F32),
            pltpu.VMEM((SEQ_DEV, KV_RANK), BF16),
            pltpu.VMEM((SEQ_DEV, ROPE_DIM), BF16),
        ),
        in_specs=[anywhere] * 21,
        out_specs=(vmem, vmem, vmem),
        scratch_shapes=scratch,
        compiler_params=pltpu.CompilerParams(
            collective_id=0, has_side_effects=True, vmem_limit_bytes=60 * 1024 * 1024
        ),
        name="layer",
    )(
        cache_lengths, route_weight.T, tokens,
        attn_gain[None, :], q_gain[None, :], kv_gain[None, :], moe_gain[None, :],
        expert_ids.T, inverse,
        cache_latent, jnp.swapaxes(cache_rope, 1, 2),
        w_qdown, w_kvdown, w_krope.T, w_qup, w_kup, w_vup, w_out,
        expert_gate, expert_up, expert_down,
    )


def solution(mesh):
    rows = P("ep", None)
    cube = P("ep", None, None)
    placed = (rows, cube, cube, P("ep"), rows, rows) + (P(),) * 11 + (cube, cube, cube)
    return jax.shard_map(
        shards,
        mesh=mesh,
        in_specs=placed,
        out_specs=(rows, rows, rows),
        check_vma=False,
    )
```
